256 devices in a mesh: grp: 2 (over y), ep: 32 (over z, core), tp: 4 (over x).
Axes of the slice: x: 4, y: 2, z: 16, core: 2. Of those that a mesh axis runs over, the one named last changes fastest.
The devices are a block of a 4x16x16 slice.
Arguments:
- outer_gate: bfloat16 [16384, 2048], P(('grp', 'ep'), 'tp'), parts along dimension 0, may hold values from -6 to 6
- inner_gate: bfloat16 [16384, 2048], P(('grp', 'ep'), 'tp'), parts along dimension 0, may hold values from -6 to 6
- inner_value: bfloat16 [16384, 2048], P(('grp', 'ep'), 'tp'), parts along dimension 0, may hold values from -6 to 6
- conv_taps: bfloat16 [3, 2048], replicated, may hold values from -3 to 3
- mixer_out: bfloat16 [2048, 2048], P('tp'), may hold values from -0.125 to 0.125
- mixer_gain: float32 [2048], replicated, may hold values from 0.1 to 1.9
- moe_tokens: bfloat16 [16384, 2048], P(('grp', 'ep', 'tp')), parts along dimension 0, may hold values from -6 to 6
- expert_gain: float32 [2048], replicated, may hold values from 0.1 to 1.9
- route_ids: int32 [16384, 4], P(('grp', 'ep', 'tp')), parts along dimension 0, may hold values from 0 to 127, all different within a row; in each aligned block of 64 rows (0 to 63, 64 to 127, ...) at most 3 rows name the same one
- route_weights: float32 [16384, 4], P(('grp', 'ep', 'tp')), parts along dimension 0, may hold values from 0.2 to 1
- expert_gate: bfloat16 [128, 2048, 512], P(('ep', 'tp')), may hold values from -0.125 to 0.125
- expert_up: bfloat16 [128, 2048, 512], P(('ep', 'tp')), may hold values from -0.125 to 0.125
- expert_down: bfloat16 [128, 512, 2048], P(('ep', 'tp')), may hold values from -0.25 to 0.25
- shared_gate: bfloat16 [2048, 512], P(None, 'tp'), may hold values from -0.125 to 0.125
- shared_up: bfloat16 [2048, 512], P(None, 'tp'), may hold values from -0.125 to 0.125
- shared_down: bfloat16 [512, 2048], P('tp'), may hold values from -0.25 to 0.25
Outputs:
- mixed_rows: bfloat16 [16384, 2048], P(('grp', 'ep', 'tp')), parts along dimension 0
- expert_rows: bfloat16 [16384, 2048], P(('grp', 'ep', 'tp')), parts along dimension 0
The draws below stay inside these ranges and needn't reach their ends.
There are 2 independent parts, one for each index of `grp`. The reference program is written for one: setup_inputs(seed, part) draws one part's arguments, and reference() takes and returns one part's arrays. A program takes and returns all parts, laid end to end along the dimension named above; an argument that names none is the same for every part. Nothing has to cross between parts.
Inputs may be any that keep to these rules, and one draw needn't show every extreme that they name: `route_ids`: each row names 4 different experts; among the 64 rows of one device (aligned blocks) no expert is named more than 3 times, a bound that some block reaches.
All inputs are finite; a program needn't handle non-finite values.
Results may differ from the reference program's by a relative error of at most 0.012.
Values may be sent and summed in bfloat16 or wider, within the bound.
No kernel may reach another device: no remote copies, remote signals or barrier semaphores. Data moves between devices by JAX's collectives and lax.ppermute only.
A program may use at most 64 MiB of HBM per device.

```python
import math
import jax
import jax.numpy as jnp
import numpy as np
from jax import lax

D = 2048
F = 512
DS = 512
TOP_K = 4
TOK_DEV = 64
EXPERTS = 128
CAP = 3
TOK_A = 8192
TOK_B = 8192
N_EP = 32
N_TP = 4


def block_scale(key, extent, pieces, low, high):
    def one(dim, blocks):
        steps = jax.random.uniform(jax.random.fold_in(jax.random.fold_in(key, 6), dim), (blocks,), jnp.float32, low / len(pieces), high / len(pieces))
        return jnp.repeat(jnp.exp(steps), extent[dim] // blocks).reshape((-1,) + (1,) * (len(extent) - dim - 1))

    gain = one(*pieces[0])
    for cut in pieces[1:]:
        gain = gain * one(*cut)
    return gain


def routed_block(key, own, number, rows, number_of, top, limit, skew):
    sequence = jax.random.permutation(key, number_of)
    packed, common = shares(number_of, rows * top, limit, skew, True), shares(number_of, rows * top, limit, skew, False)
    places = jnp.arange(number_of)

    def named(tallies, offset_by):
        used = int((tallies > 0).sum())
        fixed = max(1, used // 4)
        passed = fixed + (places - fixed + offset_by * (used - fixed)) % max(1, number_of - fixed)
        return jnp.zeros((number_of,), jnp.int32).at[sequence[jnp.where(places < fixed, places, passed)]].set(jnp.asarray(tallies, jnp.int32))

    tallies = jnp.where(number % 4 == 0, named(packed, number // 4), named(common, number - number // 4 - 1))
    mixed = jax.random.permutation(jax.random.fold_in(own, 3), number_of)
    source_of, taker = mixed[0:number_of // 2 * 2:2], mixed[1:number_of // 2 * 2:2]
    room = jnp.minimum(tallies[source_of] - 1, limit - tallies[taker]) // 2
    room = jnp.where((source_of == sequence[0]) | (taker == sequence[0]) | (tallies[taker] == 0), 0, jnp.maximum(room, 0))
    passed = jax.random.randint(jax.random.fold_in(own, 4), (number_of // 2,), 0, 1 << 20) % (room + 1)
    tallies = tallies.at[source_of].add(-passed).at[taker].add(passed)
    labels = jnp.searchsorted(jnp.cumsum(tallies), jnp.arange(rows * top), side="right").astype(jnp.int32)
    listing = labels.reshape(top, rows).T
    listing = listing[jax.random.permutation(jax.random.fold_in(own, 1), rows)]
    offset_by = jax.random.randint(jax.random.fold_in(own, 2), (rows, 1), 0, top)
    return jnp.take_along_axis(listing, (jnp.arange(top)[None, :] + offset_by) % top, axis=1)


def shares(amount, total, bound, slope, full):
    loads = [(1 << 20) // math.isqrt(rank ** slope) + 1 for rank in range(1, amount + 1)]
    largest = bound if full else min(bound, max(-(-total // amount), total * loads[0] // sum(loads)))
    least = 1 if total - largest >= amount - 1 else 0
    given, surplus = [largest] + [least] * (amount - 1), total - largest - least * (amount - 1)
    while surplus > 0:
        movable = [i for i in range(1, amount) if given[i] < largest] or [i for i in range(1, amount) if given[i] < bound]
        mass, remaining = sum([loads[i] for i in movable]), surplus
        for i in movable:
            extra = min(bound - given[i], max(1, remaining * loads[i] // mass), surplus)
            given[i] = given[i] + extra
            surplus = surplus - extra
    return np.array(given)


def centred(key, dims, deviation, bound, shards=(), kind=jnp.bfloat16):
    factor_of = block_scale(key, dims, shards, -0.22, 0.18) if shards else 1.0
    array = jax.random.normal(key, dims, jnp.float32) * deviation * factor_of
    return jnp.minimum(jnp.maximum(array, -bound), bound).astype(kind)


def setup_inputs(seed: int = 0, part: int = 0) -> dict:
    seeds = jax.random.split(jax.random.key(seed), 17)
    part_splits = jax.random.split(jax.random.fold_in(seeds[16], part), 17)
    outer_gate = centred(part_splits[0], (TOK_A, D), 1.0, 6.0, ((0, 32), (1, 4)))
    inner_gate = centred(part_splits[1], (TOK_A, D), 1.0, 6.0, ((0, 32), (1, 4)))
    inner_value = centred(part_splits[2], (TOK_A, D), 1.0, 6.0, ((0, 32), (1, 4)))
    conv_taps = centred(seeds[3], (3, D), 0.577, 3.0)
    mixer_out = centred(seeds[4], (D, D), D ** -0.5, 0.125, ((0, 4),))
    mixer_gain = jnp.clip(1.0 + 0.18 * jax.random.normal(seeds[5], (D,), jnp.float32), 0.1, 1.9)
    moe_tokens = centred(part_splits[6], (TOK_B, D), 1.0, 6.0, ((0, 128),))
    expert_gain = jnp.clip(1.0 + 0.18 * jax.random.normal(seeds[7], (D,), jnp.float32), 0.1, 1.9)
    route_ids_keys = jax.random.split(jax.random.fold_in(part_splits[8], 1), TOK_B // TOK_DEV)
    route_ids_turns = jax.random.permutation(jax.random.fold_in(part_splits[8], 3), TOK_B // TOK_DEV)
    route_ids = jax.vmap(lambda own, number: routed_block(jax.random.fold_in(part_splits[8], 2), own, number, TOK_DEV, EXPERTS, TOP_K, CAP, 2))(route_ids_keys, route_ids_turns).reshape((TOK_B, TOP_K))
    route_weights = jnp.clip(jnp.exp(math.log(1.0) - 1.609438 * jax.random.uniform(part_splits[9], (TOK_B, TOP_K), jnp.float32) ** block_scale(part_splits[9], (TOK_B, TOP_K), ((0, 128),), -0.2, 0.2)), 0.2, 1.0)
    expert_gate = centred(seeds[10], (EXPERTS, D, F), D ** -0.5, 0.125, ((0, 128),))
    expert_up = centred(seeds[11], (EXPERTS, D, F), D ** -0.5, 0.125, ((0, 128),))
    expert_down = centred(seeds[12], (EXPERTS, F, D), F ** -0.5, 0.25, ((0, 128),))
    shared_gate = centred(seeds[13], (D, DS), D ** -0.5, 0.125, ((1, 4),))
    shared_up = centred(seeds[14], (D, DS), D ** -0.5, 0.125, ((1, 4),))
    shared_down = centred(seeds[15], (DS, D), DS ** -0.5, 0.25, ((0, 4),))
    return {"outer_gate": outer_gate, "inner_gate": inner_gate, "inner_value": inner_value, "conv_taps": conv_taps, "mixer_out": mixer_out, "mixer_gain": mixer_gain, "moe_tokens": moe_tokens, "expert_gain": expert_gain, "route_ids": route_ids, "route_weights": route_weights, "expert_gate": expert_gate, "expert_up": expert_up, "expert_down": expert_down, "shared_gate": shared_gate, "shared_up": shared_up, "shared_down": shared_down}


EPSILON = 1e-06

def rms_scale(values, gains):
    return values * lax.rsqrt(lax.optimization_barrier(jnp.mean(values * values, axis=-1, keepdims=True)) + EPSILON) * gains

def reference(outer_gate, inner_gate, inner_value, conv_taps, mixer_out, mixer_gain, moe_tokens, expert_gain, route_ids, route_weights, expert_gate, expert_up, expert_down, shared_gate, shared_up, shared_down):
    kernel = conv_taps.astype(jnp.float32)
    product = inner_gate.astype(jnp.float32) * inner_value.astype(jnp.float32)
    padded = jnp.concatenate([jnp.zeros((2, product.shape[1]), jnp.float32), product], axis=0)
    filtered = kernel[0] * padded[:-2] + kernel[1] * padded[1:-1] + kernel[2] * padded[2:]
    scaled = (outer_gate.astype(jnp.float32) * filtered).astype(jnp.bfloat16)
    shard_width = D // N_TP
    summed = jnp.zeros((scaled.shape[0], D), jnp.float32)
    for shard_index in range(N_TP):
        low = shard_index * shard_width
        partial_sum = jnp.dot(scaled[:, low:low + shard_width], mixer_out[low:low + shard_width], preferred_element_type=jnp.float32)
        rounded = lax.optimization_barrier(partial_sum.astype(jnp.bfloat16))
        summed = summed + rounded.astype(jnp.float32)
    mixed_rows = rms_scale(summed, mixer_gain.astype(jnp.float32)).astype(jnp.bfloat16)
    normed = rms_scale(moe_tokens.astype(jnp.float32), expert_gain.astype(jnp.float32)).astype(jnp.bfloat16)
    token_total = normed.shape[0]
    flat_ids = route_ids.reshape(-1).astype(jnp.int32)
    onehot = (flat_ids[:, None] == jnp.arange(EXPERTS, dtype=jnp.int32)[None, :]).astype(jnp.int32)
    slot_rank = lax.optimization_barrier(jnp.sum((jnp.cumsum(onehot, axis=0, dtype=jnp.int32) - onehot) * onehot, axis=1, dtype=jnp.int32))
    token_of = jnp.arange(flat_ids.shape[0], dtype=jnp.int32) // TOP_K
    slot_count = N_EP * N_TP * CAP
    target = flat_ids * slot_count + slot_rank
    slot_token = jnp.full((EXPERTS * slot_count,), token_total, jnp.int32).at[target].set(token_of).reshape(EXPERTS, slot_count)
    slot_weight = jnp.zeros((EXPERTS * slot_count,), jnp.float32).at[target].set(route_weights.reshape(-1).astype(jnp.float32)).reshape(EXPERTS, slot_count)
    padded_rows = jnp.concatenate([normed, jnp.zeros((1, D), jnp.bfloat16)], axis=0)

    def expert_step(routed, inputs):
        gate_weight, up_weight, down_weight, tokens_here, weights_here = inputs
        chosen = padded_rows[tokens_here]
        gate_value = jnp.dot(chosen, gate_weight, preferred_element_type=jnp.float32)
        up_value = jnp.dot(chosen, up_weight, preferred_element_type=jnp.float32)
        active = (jax.nn.silu(gate_value) * up_value).astype(jnp.bfloat16)
        result = jnp.dot(active, down_weight, preferred_element_type=jnp.float32)
        result = lax.optimization_barrier(result.astype(jnp.bfloat16)).astype(jnp.float32)
        return (routed.at[tokens_here].add(weights_here[:, None] * result), None)
    routed, unused = lax.scan(expert_step, jnp.zeros((token_total + 1, D), jnp.float32), (expert_gate, expert_up, expert_down, slot_token, slot_weight))
    shared_gate_value = jnp.dot(normed, shared_gate, preferred_element_type=jnp.float32)
    shared_up_value = jnp.dot(normed, shared_up, preferred_element_type=jnp.float32)
    shared_act = (jax.nn.silu(shared_gate_value) * shared_up_value).astype(jnp.bfloat16)
    hidden_width = DS // N_TP
    shared_out = jnp.zeros((token_total, D), jnp.float32)
    for shard_index in range(N_TP):
        low = shard_index * hidden_width
        partial_sum = jnp.dot(shared_act[:, low:low + hidden_width], shared_down[low:low + hidden_width], preferred_element_type=jnp.float32)
        rounded = lax.optimization_barrier(partial_sum.astype(jnp.bfloat16))
        shared_out = shared_out + rounded.astype(jnp.float32)
    expert_rows = (routed[:token_total] + shared_out).astype(jnp.bfloat16)
    return (mixed_rows, expert_rows)
```

```python
import jax
import jax.numpy as jnp
from jax import lax
from jax.sharding import PartitionSpec as P

EPSILON = 1e-06


def passed_along(array, axis, by):
    size = lax.axis_size(axis)
    pairs = [(i, i + by) for i in range(size) if 0 <= i + by < size]
    return lax.ppermute(array, axis, pairs)


def laid_out(pieces, dim):
    shape = list(pieces.shape[1:])
    shape[dim] *= pieces.shape[0]
    return jnp.moveaxis(pieces, 0, dim).reshape(shape)


def work_in_pieces(array, axis, dim, apply, out_dim):
    size, span = (lax.axis_size(axis), array.shape[dim])
    count = 2 if span % 2 == 0 else 1
    outs, length = ([], span // count)
    for k in range(count):
        share = lax.slice_in_dim(array, k * length, (k + 1) * length, axis=dim)
        starts = jnp.arange(size) * span + k * length
        outs.append(jax.vmap(apply)(lax.all_gather(share, axis), starts))
    return laid_out(jnp.concatenate(outs, axis=out_dim + 1), out_dim)


def in_blocks(array, dim, size):
    shape = array.shape
    pieces = array.reshape(*shape[:dim], size, shape[dim] // size, *shape[dim + 1 :])
    return jnp.moveaxis(pieces, dim, 0)


def summed_on_arrival(array, axis, dim):
    size = lax.axis_size(axis)
    pieces = in_blocks(array, dim, size)
    own = lax.axis_index(axis)
    total = jnp.take(pieces, own, axis=0).astype(jnp.float32)
    for k in range(1, size):
        going = jnp.take(pieces, (own + k) % size, axis=0)
        total = total + lax.ppermute(
            going, axis, [(i, (i + k) % size) for i in range(size)]
        ).astype(jnp.float32)
    return total


LANES = 128


def exchanged(rows, expert_count, capacity):
    width = rows.shape[-1]
    cut = rows.reshape(expert_count, capacity * width // LANES, LANES)
    cut = lax.all_to_all(cut, ("ep", "tp"), split_axis=0, concat_axis=0, tiled=True)
    return cut.reshape(expert_count * capacity, width)


def rms_scale(values, gains):
    return values * lax.rsqrt(jnp.mean(values * values, axis=-1, keepdims=True) + EPSILON) * gains


def on_device(
    outer_gate,
    inner_gate,
    inner_value,
    conv_taps,
    mixer_out,
    mixer_gain,
    moe_tokens,
    expert_gain,
    route_ids,
    route_weights,
    expert_gate,
    expert_up,
    expert_down,
    shared_gate,
    shared_up,
    shared_down,
):
    columns = inner_gate.shape[1]
    kernel = lax.dynamic_slice_in_dim(conv_taps, lax.axis_index("tp") * columns, columns, 1).astype(
        jnp.float32
    )
    before_gate, before_value = passed_along((inner_gate[-2:], inner_value[-2:]), "ep", 1)
    gate_rows = jnp.concatenate([before_gate, inner_gate], axis=0).astype(jnp.float32)
    value_rows = jnp.concatenate([before_value, inner_value], axis=0).astype(jnp.float32)
    product = gate_rows * value_rows
    filtered = kernel[0] * product[:-2] + kernel[1] * product[1:-1] + kernel[2] * product[2:]
    scaled = (outer_gate.astype(jnp.float32) * filtered).astype(jnp.bfloat16)
    normed = rms_scale(moe_tokens.astype(jnp.float32), expert_gain).astype(jnp.bfloat16)
    feature_width = normed.shape[1]

    def shared_piece(piece, start):
        gate_value = jnp.dot(piece, shared_gate, preferred_element_type=jnp.float32)
        up_value = jnp.dot(piece, shared_up, preferred_element_type=jnp.float32)
        return (jax.nn.silu(gate_value) * up_value).astype(jnp.bfloat16)

    shared_act = work_in_pieces(normed, "tp", 0, shared_piece, 0)
    mixer_part = jnp.dot(scaled, mixer_out, preferred_element_type=jnp.float32)
    shared_part = jnp.dot(shared_act, shared_down, preferred_element_type=jnp.float32)
    both_sums = summed_on_arrival(
        jnp.concatenate([mixer_part, shared_part], axis=1).astype(jnp.bfloat16), "tp", 0
    )
    mixed_rows = rms_scale(both_sums[:, :feature_width], mixer_gain).astype(jnp.bfloat16)
    shared_out = both_sums[:, feature_width:]
    row_count, top_count = route_ids.shape
    ep_count = lax.axis_size("ep")
    tp_count = lax.axis_size("tp")
    expert_count = ep_count * tp_count
    capacity = (3 * row_count * top_count + 2 * expert_count - 1) // (2 * expert_count)
    flat_ids = route_ids.reshape(-1)
    onehot = (flat_ids[:, None] == jnp.arange(expert_count, dtype=jnp.int32)[None, :]).astype(
        jnp.int32
    )
    slot_rank = jnp.sum(
        (jnp.cumsum(onehot, axis=0, dtype=jnp.int32) - onehot) * onehot, axis=1, dtype=jnp.int32
    )
    target = flat_ids * capacity + slot_rank
    token_of = jnp.arange(flat_ids.shape[0], dtype=jnp.int32) // top_count
    slot_token = jnp.zeros((expert_count * capacity,), jnp.int32).at[target].set(token_of)
    flat_in = exchanged(normed[slot_token], expert_count, capacity)
    gate_value = jnp.dot(flat_in, expert_gate[0], preferred_element_type=jnp.float32)
    up_value = jnp.dot(flat_in, expert_up[0], preferred_element_type=jnp.float32)
    active = (jax.nn.silu(gate_value) * up_value).astype(jnp.bfloat16)
    result = jnp.dot(active, expert_down[0], preferred_element_type=jnp.float32).astype(
        jnp.bfloat16
    )
    returned = exchanged(result, expert_count, capacity)
    picked = returned[target].astype(jnp.float32)
    weights = route_weights.reshape(-1)
    routed = jnp.sum(
        (weights[:, None] * picked).reshape(row_count, top_count, feature_width), axis=1
    )
    expert_rows = (shared_out + routed).astype(jnp.bfloat16)
    return (mixed_rows, expert_rows)


def solution(mesh):
    return jax.shard_map(
        on_device,
        mesh=mesh,
        in_specs=(
            P(("grp", "ep"), "tp"),
            P(("grp", "ep"), "tp"),
            P(("grp", "ep"), "tp"),
            P(),
            P("tp", None),
            P(),
            P(("grp", "ep", "tp"), None),
            P(),
            P(("grp", "ep", "tp"), None),
            P(("grp", "ep", "tp"), None),
            P(("ep", "tp"), None, None),
            P(("ep", "tp"), None, None),
            P(("ep", "tp"), None, None),
            P(None, "tp"),
            P(None, "tp"),
            P("tp", None),
        ),
        out_specs=(P(("grp", "ep", "tp"), None), P(("grp", "ep", "tp"), None)),
        check_vma=False,
    )
```

```python
import functools
import jax
import jax.numpy as jnp
from jax import lax
from jax.experimental import pallas as pl
from jax.experimental.pallas import tpu as pltpu
from jax.sharding import PartitionSpec as P

EPSILON = 1e-06
LANES = 128
CORES = 2
F32 = jnp.float32
BF16 = jnp.bfloat16
I32 = jnp.int32
VMEM = pl.BlockSpec(memory_space=pltpu.VMEM)
PARAMS = pltpu.CompilerParams(vmem_limit_bytes=40 * 1024 * 1024)


def on_core(body, shapes, *args, scratch=()):
    single = not isinstance(shapes, (list, tuple))
    out = [shapes] if single else list(shapes)
    got = pl.pallas_call(
        body,
        out_shape=[jax.ShapeDtypeStruct(s, t) for s, t in out],
        in_specs=[VMEM] * len(args),
        out_specs=[VMEM] * len(out),
        scratch_shapes=list(scratch),
        compiler_params=PARAMS,
    )(*args)
    return got[0] if single else got


def ring(size, by):
    return [(i, (i + by) % size) for i in range(size)]


def cut_rows(rows):
    return -(-rows // 8) * 8


def prepare_kernel(tokens, gain, ids, weights, left, right, normed):
    half = right.shape[1]
    values = tokens[...].astype(F32)
    scale = lax.rsqrt(jnp.mean(values * values, axis=-1, keepdims=True) + EPSILON)
    rows = (values * scale * gain[...]).astype(BF16)
    normed[...] = rows
    left[:, :half] = rows[:, :half]
    right[...] = rows[:, half:]
    count, top = ids.shape
    lane = lax.broadcasted_iota(I32, (count, LANES), 1)
    picks = [lane == ids[:, k : k + 1] for k in range(top)]
    named = functools.reduce(jnp.logical_or, picks).astype(F32).astype(BF16)
    before = (
        lax.broadcasted_iota(I32, (count, count), 1) < lax.broadcasted_iota(I32, (count, count), 0)
    ).astype(F32).astype(BF16)
    seen = jnp.dot(before, named, preferred_element_type=F32)
    facts = jnp.zeros((count, LANES), F32)
    for k in range(top):
        rank = jnp.sum(jnp.where(picks[k], seen, 0.0), axis=1, keepdims=True)
        weight = weights[:, k : k + 1]
        high = weight.astype(BF16).astype(F32)
        named_id = ids[:, k : k + 1].astype(F32)
        for place, value in enumerate((named_id, rank, high, weight - high)):
            facts = jnp.where(lane == place * top + k, value, facts)
    left[:, half:] = facts.astype(BF16)


def slot_rows(facts, block, top, cap, per_place, tp_count):
    ep, tp = lax.axis_index("ep"), lax.axis_index("tp")
    ids = facts[:, :top].astype(I32)
    ranks = facts[:, top : 2 * top].astype(I32)
    at = ids // tp_count
    across = jnp.bitwise_xor(at, ep) % CORES
    along = (ids % tp_count - tp + tp_count) % tp_count
    row = (across * tp_count + along) * per_place + block * cap + ranks
    return jnp.where(at // CORES == ep // CORES, row, -1)


def pick_kernel(top, cap, tp_count, blocks, rows, *refs):
    lefts, rights = refs[:blocks], refs[blocks : 2 * blocks]
    places = tp_count * CORES
    outs = refs[2 * blocks : 2 * blocks + places]
    held, chosen = refs[2 * blocks + places :]
    per_place = cut_rows(rows)
    count, half = rights[0].shape
    lane = lax.broadcasted_iota(I32, (count, chosen.shape[1]), 1)
    for b in range(blocks):
        span = pl.ds(b * count, count)
        held[span, :half] = lefts[b][:, :half]
        held[span, half:] = rights[b][...]
        row = slot_rows(lefts[b][:, half:].astype(F32), b, top, cap, per_place, tp_count)
        hit = functools.reduce(
            jnp.logical_or, [lane == row[:, k : k + 1] for k in range(top)]
        )
        chosen[span, :] = hit.astype(F32).astype(BF16)
    got = lax.dot_general(
        chosen[...], held[...], (((0,), (0,)), ((), ())), preferred_element_type=F32
    )
    for j in range(places):
        outs[j][...] = got[j * per_place : j * per_place + rows].astype(BF16)


def expert_kernel(places, rows, *refs):
    pieces, (gate, up, down) = refs[:places], refs[places : places + 3]
    outs, held = refs[places + 3 : 2 * places + 3], refs[2 * places + 3]
    per_place = cut_rows(rows)
    for j in range(places):
        held[j * per_place : j * per_place + rows, :] = pieces[j][...]
    gate_value = jnp.dot(held[...], gate[0], preferred_element_type=F32)
    up_value = jnp.dot(held[...], up[0], preferred_element_type=F32)
    active = (gate_value / (1.0 + jnp.exp(-gate_value)) * up_value).astype(BF16)
    result = jnp.dot(active, down[0], preferred_element_type=F32)
    for j in range(places):
        outs[j][...] = result[j * per_place : j * per_place + rows].astype(BF16)


def combine_kernel(top, cap, tp_count, blocks, rows, *refs):
    places = tp_count * CORES
    pieces, lefts = refs[:places], refs[places : places + blocks]
    outs = refs[places + blocks : places + 3 * blocks]
    held = refs[-1]
    per_place = cut_rows(rows)
    if per_place != rows:
        held[...] = jnp.zeros_like(held)
    for j in range(places):
        held[j * per_place : j * per_place + rows, :] = pieces[j][...]
    half = outs[0].shape[1]
    count = lefts[0].shape[0]
    lane = lax.broadcasted_iota(I32, (count, held.shape[0]), 1)
    for b in range(blocks):
        facts = lefts[b][:, half:].astype(F32)
        row = slot_rows(facts, b, top, cap, per_place, tp_count)
        high = jnp.zeros(lane.shape, F32)
        low = jnp.zeros(lane.shape, F32)
        for k in range(top):
            hit = lane == row[:, k : k + 1]
            high = jnp.where(hit, facts[:, 2 * top + k : 2 * top + k + 1], high)
            low = jnp.where(hit, facts[:, 3 * top + k : 3 * top + k + 1], low)
        part = jnp.dot(high.astype(BF16), held[...], preferred_element_type=F32)
        part = part + jnp.dot(low.astype(BF16), held[...], preferred_element_type=F32)
        outs[2 * b][...] = part[:, :half].astype(BF16)
        outs[2 * b + 1][...] = part[:, half:].astype(BF16)


def rms_scale(values, gains):
    return values * lax.rsqrt(jnp.mean(values * values, axis=-1, keepdims=True) + EPSILON) * gains


def on_device(
    outer_gate,
    inner_gate,
    inner_value,
    conv_taps,
    mixer_out,
    mixer_gain,
    moe_tokens,
    expert_gain,
    route_ids,
    route_weights,
    expert_gate,
    expert_up,
    expert_down,
    shared_gate,
    shared_up,
    shared_down,
):
    ep_count, tp_count = lax.axis_size("ep"), lax.axis_size("tp")
    ep, tp = lax.axis_index("ep"), lax.axis_index("tp")
    row_count, width = moe_tokens.shape
    top = route_ids.shape[1]
    half = width // 2
    expert_count = ep_count * tp_count
    cap = (3 * row_count * top + 2 * expert_count - 1) // (2 * expert_count)
    chips = ep_count // CORES
    reach = chips // 2

    left, right, normed = on_core(
        prepare_kernel,
        [((row_count, half + LANES), BF16), ((row_count, half), BF16), ((row_count, width), BF16)],
        moe_tokens,
        expert_gain.reshape(1, width),
        route_ids,
        route_weights,
    )

    rise, fall = ring(ep_count, CORES), ring(ep_count, -CORES)
    got = {("u", 0): (left, right), ("d", 0): (left, right)}
    order = [("u", 0)]
    for s in range(1, reach + 1):
        got["u", s] = tuple(lax.ppermute(v, "ep", rise) for v in got["u", s - 1])
        order.append(("u", s))
        if s < chips - reach:
            got["d", s] = tuple(lax.ppermute(v, "ep", fall) for v in got["d", s - 1])
            order.append(("d", s))
    order = order[:-1] if len(order) > chips else order
    cuts = [0, chips // 2, 3 * chips // 4, chips]
    places = [(across, along) for across in range(CORES) for along in range(tp_count)]
    whole = [(i, j) for i in range(ep_count) for j in range(tp_count)]

    def moved(piece, across, along, back=False):
        if not across and not along:
            return piece
        pairs = [
            (i * tp_count + j, (i ^ across) * tp_count + (j + along) % tp_count)
            for i, j in whole
        ]
        if back:
            pairs = [(b, a) for a, b in pairs]
        return lax.ppermute(piece, ("ep", "tp"), pairs)

    near = [normed] + [lax.ppermute(normed, "tp", ring(tp_count, k)) for k in range(1, tp_count)]

    parts = {}
    for low, high in zip(cuts[:-1], cuts[1:]):
        names = order[low:high]
        blocks = len(names)
        rows = blocks * cap
        slots = cut_rows(rows) * len(places)
        lefts = [got[n][0] for n in names]
        rights = [got[n][1] for n in names]
        going = on_core(
            functools.partial(pick_kernel, top, cap, tp_count, blocks, rows),
            [((rows, width), BF16)] * len(places),
            *lefts,
            *rights,
            scratch=[
                pltpu.VMEM((blocks * row_count, width), BF16),
                pltpu.VMEM((blocks * row_count, slots), BF16),
            ],
        )
        here = [moved(v, *place) for v, place in zip(going, places)]
        result = on_core(
            functools.partial(expert_kernel, len(places), rows),
            [((rows, width), BF16)] * len(places),
            *here,
            expert_gate,
            expert_up,
            expert_down,
            scratch=[pltpu.VMEM((slots, width), BF16)],
        )
        home = [moved(v, *place, back=True) for v, place in zip(result, places)]
        done = on_core(
            functools.partial(combine_kernel, top, cap, tp_count, blocks, rows),
            [((row_count, half), BF16)] * (2 * blocks),
            *home,
            *lefts,
            scratch=[pltpu.VMEM((slots, width), BF16)],
        )
        for b, n in enumerate(names):
            parts[n] = (done[2 * b], done[2 * b + 1])

    columns = inner_gate.shape[1]
    kernel = lax.dynamic_slice_in_dim(conv_taps, tp * columns, columns, 1).astype(F32)
    pairs = [(i, i + 1) for i in range(ep_count - 1)]
    before_gate, before_value = lax.ppermute((inner_gate[-2:], inner_value[-2:]), "ep", pairs)
    gate_rows = jnp.concatenate([before_gate, inner_gate], axis=0).astype(F32)
    value_rows = jnp.concatenate([before_value, inner_value], axis=0).astype(F32)
    product = gate_rows * value_rows
    filtered = kernel[0] * product[:-2] + kernel[1] * product[1:-1] + kernel[2] * product[2:]
    scaled = (outer_gate.astype(F32) * filtered).astype(BF16)
    mixer_part = jnp.dot(scaled, mixer_out, preferred_element_type=F32).astype(BF16)
    mixer_part = mixer_part.reshape(tp_count, row_count, width)
    mixed = jnp.take(mixer_part, tp, axis=0).astype(F32)
    for k in range(1, tp_count):
        piece = jnp.take(mixer_part, (tp + k) % tp_count, axis=0)
        mixed = mixed + lax.ppermute(piece, "tp", ring(tp_count, k)).astype(F32)
    mixed_rows = rms_scale(mixed, mixer_gain).astype(BF16)

    all_rows = jnp.concatenate(near, axis=0)
    gate_value = jnp.dot(all_rows, shared_gate, preferred_element_type=F32)
    up_value = jnp.dot(all_rows, shared_up, preferred_element_type=F32)
    shared_act = (jax.nn.silu(gate_value) * up_value).astype(BF16)
    shared_part = jnp.dot(shared_act, shared_down, preferred_element_type=F32).astype(BF16)
    shared = shared_part[:row_count].astype(F32)
    for k in range(1, tp_count):
        piece = shared_part[k * row_count : (k + 1) * row_count]
        shared = shared + lax.ppermute(piece, "tp", ring(tp_count, -k)).astype(F32)

    sums = []
    for h in range(2):
        a, b = parts["u", reach][h], parts["u", chips - reach - 1][h]
        for s in range(reach - 1, -1, -1):
            a = lax.ppermute(a, "ep", rise)
            a = a + parts["d", s][h] if s else a
        for s in range(chips - reach - 2, -1, -1):
            b = lax.ppermute(b, "ep", fall)
            b = b + parts["u", s][h] if s else b
        sums.append(a.astype(F32) + b.astype(F32) + parts["u", 0][h].astype(F32))
    expert_rows = (shared + jnp.concatenate(sums, axis=1)).astype(BF16)
    return (mixed_rows, expert_rows)


def solution(mesh):
    return jax.shard_map(
        on_device,
        mesh=mesh,
        in_specs=(
            P(("grp", "ep"), "tp"),
            P(("grp", "ep"), "tp"),
            P(("grp", "ep"), "tp"),
            P(),
            P("tp", None),
            P(),
            P(("grp", "ep", "tp"), None),
            P(),
            P(("grp", "ep", "tp"), None),
            P(("grp", "ep", "tp"), None),
            P(("ep", "tp"), None, None),
            P(("ep", "tp"), None, None),
            P(("ep", "tp"), None, None),
            P(None, "tp"),
            P(None, "tp"),
            P("tp", None),
        ),
        out_specs=(P(("grp", "ep", "tp"), None), P(("grp", "ep", "tp"), None)),
        check_vma=False,
    )
```

```python
import functools
import jax
import jax.numpy as jnp
from jax import lax
from jax.experimental import pallas as pl
from jax.experimental.pallas import tpu as pltpu
from jax.sharding import PartitionSpec as P

EPSILON = 1e-06
LANES = 128
CORES = 2
F32 = jnp.float32
BF16 = jnp.bfloat16
I32 = jnp.int32
MIB = 1024 * 1024
VMEM = pl.BlockSpec(memory_space=pltpu.VMEM)
HBM = pl.BlockSpec(memory_space=pltpu.HBM)
AUTO = pl.BlockSpec()


def on_core(body, ins, outs, *args, scratch=(), limit=16):
    return pl.pallas_call(
        body,
        out_shape=[jax.ShapeDtypeStruct(s, t) for s, t, _ in outs],
        in_specs=ins,
        out_specs=[where for _, _, where in outs],
        scratch_shapes=list(scratch),
        compiler_params=pltpu.CompilerParams(vmem_limit_bytes=limit * MIB),
    )(*args)


def ring(size, by):
    return [(i, (i + by) % size) for i in range(size)]


def prepare_kernel(tokens, gain, ids, weights, left, right, normed):
    half = right.shape[1]
    values = tokens[...].astype(F32)
    scale = lax.rsqrt(jnp.mean(values * values, axis=-1, keepdims=True) + EPSILON)
    rows = (values * scale * gain[...]).astype(BF16)
    normed[...] = rows
    left[:, :half] = rows[:, :half]
    right[...] = rows[:, half:]
    top, count = ids.shape
    most = weights[...].astype(BF16).astype(F32)
    lists = jnp.concatenate([ids[...].astype(F32), most, weights[...] - most], axis=0)
    above = lax.broadcasted_iota(I32, (count, count), 1)
    below = lax.broadcasted_iota(I32, (count, count), 0)
    same = (above == below).astype(F32).astype(BF16)
    turned = lax.dot_general(
        same, lists.astype(BF16), (((1,), (1,)), ((), ())), preferred_element_type=F32
    )
    lane = lax.broadcasted_iota(I32, (count, LANES), 1)
    named_ids = turned[:, :top].astype(I32)
    picks = [lane == named_ids[:, k : k + 1] for k in range(top)]
    named = functools.reduce(jnp.logical_or, picks).astype(F32).astype(BF16)
    before = (above < below).astype(F32).astype(BF16)
    seen = jnp.dot(before, named, preferred_element_type=F32)
    facts = jnp.zeros((count, LANES), F32)
    for k in range(top):
        rank = jnp.sum(jnp.where(picks[k], seen, 0.0), axis=1, keepdims=True)
        columns = (turned[:, k : k + 1], rank) + tuple(
            turned[:, i * top + k : i * top + k + 1] for i in (1, 2)
        )
        for place, value in enumerate(columns):
            facts = jnp.where(lane == place * top + k, value, facts)
    left[:, half:] = facts.astype(BF16)


def slot_rows(facts, block, top, cap, per_place, tp_count):
    ids = facts[:, :top].astype(I32)
    ranks = facts[:, top : 2 * top].astype(I32)
    here = lax.axis_index("z") * CORES + lax.axis_index("core")
    at = ids // tp_count
    across = (at + here) % CORES
    along = (ids % tp_count - lax.axis_index("tp") + tp_count) % tp_count
    row = (across * tp_count + along) * per_place + block * cap + ranks
    return jnp.where(at // CORES == lax.axis_index("z"), row, -1)


def pick_kernel(top, cap, tp_count, groups, blocks, *refs):
    total, plane = groups * blocks, CORES * tp_count
    lefts, rights = refs[:total], refs[total : 2 * total]
    slots = refs[2 * total : 2 * total + plane]
    facts, held, chosen, arrived = refs[2 * total + plane :]
    count, half = rights[0].shape
    per_place = blocks * cap
    copies = []
    for b in range(total):
        span = pl.ds(b * count, count)
        copies.append(
            (
                pltpu.make_async_copy(
                    lefts[b].at[:, pl.ds(half, LANES)], facts.at[span, :], arrived.at[0, b]
                ),
                pltpu.make_async_copy(
                    lefts[b].at[:, pl.ds(0, half)], held.at[span, pl.ds(0, half)], arrived.at[1, b]
                ),
                pltpu.make_async_copy(
                    rights[b], held.at[span, pl.ds(half, half)], arrived.at[2, b]
                ),
            )
        )
    for trio in copies:
        for copy in trio:
            copy.start()
    wide = groups_lanes(plane * per_place)
    pair = LANES // count
    lane = lax.broadcasted_iota(I32, (count, wide), 1)
    for first in range(0, total, pair):
        hits = []
        for b in range(first, first + pair):
            copies[b][0].wait()
            known = facts[pl.ds(b * count, count), :].astype(F32)
            row = slot_rows(known, b % blocks, top, cap, per_place, tp_count)
            hit = functools.reduce(
                jnp.logical_or, [lane == row[:, k : k + 1] for k in range(top)]
            )
            hits.append(hit.astype(F32))
        turned = jnp.transpose(jnp.concatenate(hits, axis=0)).astype(BF16)
        g, at = first // blocks, first % blocks * count
        chosen[g, :, at : at + pair * count] = turned[: plane * per_place]
    for trio in copies:
        trio[1].wait()
        trio[2].wait()
    step = 512

    def columns(n, unused):
        span = pl.ds(pl.multiple_of(n * step, step), step)
        for g in range(groups):
            rows = held[pl.ds(g * blocks * count, blocks * count), span]
            got = jnp.dot(chosen[g], rows, preferred_element_type=F32).astype(BF16)
            for j in range(plane):
                slots[j][g * per_place : (g + 1) * per_place, span] = got[
                    j * per_place : (j + 1) * per_place
                ]
        return unused

    lax.fori_loop(0, 2 * half // step, columns, 0)


def groups_lanes(rows):
    return -(-rows // LANES) * LANES


def load_kernel(*refs):
    count = len(refs) // 2
    arrived = refs[-1]
    copies = [
        pltpu.make_async_copy(refs[i].at[0], refs[count + i], arrived.at[i]) for i in range(count)
    ]
    for copy in copies:
        copy.start()
    for copy in copies:
        copy.wait()


def expert_kernel(plane, rows, *refs):
    pieces, (gate, up, down) = refs[:plane], refs[plane : plane + 3]
    outs = refs[plane + 3 : 2 * plane + 3]
    held, active = refs[2 * plane + 3 :]
    for j in range(plane):
        held[j * rows : (j + 1) * rows, :] = pieces[j][...]
    step = 256

    def hide(n, unused):
        span = pl.ds(pl.multiple_of(n * step, step), step)
        gate_value = jnp.dot(held[...], gate[:, span], preferred_element_type=F32)
        up_value = jnp.dot(held[...], up[:, span], preferred_element_type=F32)
        active[:, span] = (gate_value / (1.0 + jnp.exp(-gate_value)) * up_value).astype(BF16)
        return unused

    lax.fori_loop(0, gate.shape[1] // step, hide, 0)

    def show(n, unused):
        span = pl.ds(pl.multiple_of(n * step, step), step)
        got = jnp.dot(active[...], down[:, span], preferred_element_type=F32).astype(BF16)
        for j in range(plane):
            outs[j][:, span] = got[j * rows : (j + 1) * rows]
        return unused

    lax.fori_loop(0, down.shape[1] // step, show, 0)


def sides_kernel(tp_count, *refs):
    outer_gate, inner_gate, inner_value, before, taps, mixer_out = refs[:6]
    near, (gate, up, down) = refs[6 : 6 + tp_count], refs[6 + tp_count : 9 + tp_count]
    outs = refs[9 + tp_count : 9 + 2 * tp_count]
    product, scaled, held = refs[9 + 2 * tp_count :]
    rows, columns = inner_gate.shape
    count, width = near[0].shape
    tp = lax.axis_index("tp")
    halo = before.shape[0] // 2
    lead = product.shape[0] - rows
    earlier = before[...].astype(F32)
    product[lead - halo : lead, :] = earlier[:halo] * earlier[halo:]
    product[lead:, :] = inner_gate[...].astype(F32) * inner_value[...].astype(F32)
    tap = taps[:, pl.ds(pl.multiple_of(tp * columns, columns), columns)].astype(F32)
    filtered = tap[0:1] * product[lead - 2 : lead - 2 + rows, :]
    filtered = filtered + tap[1:2] * product[lead - 1 : lead - 1 + rows, :]
    filtered = filtered + tap[2:3] * product[lead : lead + rows, :]
    product[lead:, :] = outer_gate[...].astype(F32) * filtered
    for k in range(tp_count):
        at = pl.multiple_of((tp + k) % tp_count * count, count)
        scaled[k * count : (k + 1) * count, :] = product[pl.ds(lead + at, count), :].astype(BF16)
        held[k * count : (k + 1) * count, :] = near[-k % tp_count][...]
    gate_value = jnp.dot(held[...], gate[...], preferred_element_type=F32)
    up_value = jnp.dot(held[...], up[...], preferred_element_type=F32)
    active = (gate_value / (1.0 + jnp.exp(-gate_value)) * up_value).astype(BF16)
    step = 512

    def columns_of(n, unused):
        at = pl.multiple_of(n * step, step)
        mixed = jnp.dot(scaled[...], mixer_out[:, pl.ds(at, step)], preferred_element_type=F32)
        shared = jnp.dot(active, down[:, pl.ds(at, step)], preferred_element_type=F32)
        for k in range(tp_count):
            own = slice(k * count, (k + 1) * count)
            outs[k][:, pl.ds(at, step)] = mixed[own].astype(BF16)
            outs[k][:, pl.ds(width + at, step)] = shared[own].astype(BF16)
        return unused

    lax.fori_loop(0, width // step, columns_of, 0)


def combine_kernel(top, cap, tp_count, group, blocks, *refs):
    plane = CORES * tp_count
    back, facts = refs[:plane], refs[plane]
    outs = refs[plane + 1 : plane + 1 + 2 * blocks]
    held, high, low = refs[plane + 1 + 2 * blocks :]
    per_place = blocks * cap
    for j in range(plane):
        held[j * per_place : (j + 1) * per_place, :] = back[j][
            group * per_place : (group + 1) * per_place, :
        ]
    count, half = outs[0].shape
    lane = lax.broadcasted_iota(I32, (count, plane * per_place), 1)
    for b in range(blocks):
        known = facts[pl.ds((group * blocks + b) * count, count), :].astype(F32)
        row = slot_rows(known, b, top, cap, per_place, tp_count)
        most = jnp.zeros(lane.shape, F32)
        rest = jnp.zeros(lane.shape, F32)
        for k in range(top):
            hit = lane == row[:, k : k + 1]
            most = jnp.where(hit, known[:, 2 * top + k : 2 * top + k + 1], most)
            rest = jnp.where(hit, known[:, 3 * top + k : 3 * top + k + 1], rest)
        high[pl.ds(b * count, count), :] = most.astype(BF16)
        low[pl.ds(b * count, count), :] = rest.astype(BF16)
    step = 512
    for h in range(2):

        def columns(n, unused):
            at = pl.multiple_of(n * step, step)
            rows = held[:, pl.ds(h * half + at, step)]
            part = jnp.dot(high[...], rows, preferred_element_type=F32)
            part = part + jnp.dot(low[...], rows, preferred_element_type=F32)
            part = part.astype(BF16)
            for b in range(blocks):
                outs[2 * b + h][:, pl.ds(at, step)] = part[b * count : (b + 1) * count]
            return unused

        lax.fori_loop(0, half // step, columns, 0)


def plane_exchange(pieces, chips, tp_count):
    whole = [(z, core, i) for z in range(chips) for core in range(CORES) for i in range(tp_count)]

    def moved(piece, across, along):
        pairs = [
            (
                (z * CORES + core) * tp_count + i,
                (z * CORES + (core ^ across)) * tp_count + (i + along) % tp_count,
            )
            for z, core, i in whole
        ]
        return lax.ppermute(piece, ("z", "core", "tp"), pairs)

    middle = tp_count // 2
    halfway = [moved(pieces[middle], 0, 1), moved(pieces[tp_count + middle], 0, -1)]
    got = {0: pieces[0]}
    for along in (1, tp_count - 1):
        for across in range(CORES):
            got[across * tp_count + along] = moved(pieces[across * tp_count + along], across, along)
    got[tp_count] = moved(pieces[tp_count], 1, 0)
    got[middle] = moved(halfway[0], 0, middle - 1)
    got[tp_count + middle] = moved(halfway[1], 1, 1 - middle)
    return [got[j] for j in range(CORES * tp_count)]


def rms_scale(values, gains):
    return values * lax.rsqrt(jnp.mean(values * values, axis=-1, keepdims=True) + EPSILON) * gains


def on_device(
    outer_gate,
    inner_gate,
    inner_value,
    conv_taps,
    mixer_out,
    mixer_gain,
    moe_tokens,
    expert_gain,
    route_ids,
    route_weights,
    expert_gate,
    expert_up,
    expert_down,
    shared_gate,
    shared_up,
    shared_down,
):
    chips, tp_count = lax.axis_size("z"), lax.axis_size("tp")
    plane = CORES * tp_count
    tp = lax.axis_index("tp")
    row_count, width = moe_tokens.shape
    top = route_ids.shape[1]
    half = width // 2
    expert_count = chips * plane
    cap = (3 * row_count * top + 2 * expert_count - 1) // (2 * expert_count)
    reach = chips // 2
    far = chips - reach - 1

    left, right, normed = on_core(
        prepare_kernel,
        [AUTO] * 4,
        [
            ((row_count, half + LANES), BF16, VMEM),
            ((row_count, half), BF16, VMEM),
            ((row_count, width), BF16, VMEM),
        ],
        moe_tokens,
        expert_gain.reshape(1, width),
        route_ids.T,
        route_weights.T,
        limit=56,
    )

    rise, fall = ring(chips, 1), ring(chips, -1)
    got = {("u", 0): (left, right), ("d", 0): (left, right)}
    order = [("u", 0)]
    for s in range(1, reach + 1):
        got["u", s] = tuple(lax.ppermute(v, "z", rise) for v in got["u", s - 1])
        order.append(("u", s))
        if s <= far:
            got["d", s] = tuple(lax.ppermute(v, "z", fall) for v in got["d", s - 1])
            order.append(("d", s))

    groups = 2
    blocks = chips // groups
    rows = chips * cap
    lefts = [got[n][0] for n in order]
    rights = [got[n][1] for n in order]
    *slots, facts = on_core(
        functools.partial(pick_kernel, top, cap, tp_count, groups, blocks),
        [HBM] * (2 * chips),
        [((rows, width), BF16, VMEM)] * plane + [((chips * row_count, LANES), BF16, VMEM)],
        *lefts,
        *rights,
        scratch=[
            pltpu.VMEM((chips * row_count, width), BF16),
            pltpu.VMEM((groups, plane * blocks * cap, blocks * row_count), BF16),
            pltpu.SemaphoreType.DMA((3, chips)),
        ],
        limit=12,
    )
    last, normed, loads, slots = lax.optimization_barrier(
        (
            jnp.concatenate([inner_gate[-2:], inner_value[-2:]], axis=0),
            normed,
            (expert_gate, expert_up, expert_down),
            slots,
        )
    )
    here = plane_exchange(slots, chips, tp_count)
    hidden = expert_gate.shape[2]
    gate, up, down = on_core(
        load_kernel,
        [HBM] * 3,
        [((width, hidden), BF16, VMEM), ((width, hidden), BF16, VMEM), ((hidden, width), BF16, VMEM)],
        *loads,
        scratch=[pltpu.SemaphoreType.DMA((3,))],
        limit=52,
    )

    one = lax.ppermute(normed, "tp", ring(tp_count, 1))
    back_one = lax.ppermute(normed, "tp", ring(tp_count, -1))
    two = jnp.concatenate(
        [
            lax.ppermute(one[:, :half], "tp", ring(tp_count, 1)),
            lax.ppermute(back_one[:, half:], "tp", ring(tp_count, -1)),
        ],
        axis=1,
    )
    near = [normed, one, two, back_one]
    pairs = [(i, i + 1) for i in range(chips * CORES - 1)]
    before = lax.ppermute(last, ("z", "core"), pairs)

    result = on_core(
        functools.partial(expert_kernel, plane, rows),
        [VMEM] * (plane + 3),
        [((rows, width), BF16, VMEM)] * plane,
        *here,
        gate,
        up,
        down,
        scratch=[
            pltpu.VMEM((plane * rows, width), BF16),
            pltpu.VMEM((plane * rows, hidden), BF16),
        ],
        limit=10,
    )
    turned = [result[a * tp_count + -k % tp_count] for a in range(CORES) for k in range(tp_count)]
    turned = plane_exchange(turned, chips, tp_count)
    back = [turned[a * tp_count + -k % tp_count] for a in range(CORES) for k in range(tp_count)]

    columns = inner_gate.shape[1]
    both = on_core(
        functools.partial(sides_kernel, tp_count),
        [VMEM] * (9 + tp_count),
        [((row_count, 2 * width), BF16, VMEM)] * tp_count,
        outer_gate,
        inner_gate,
        inner_value,
        before,
        conv_taps,
        mixer_out,
        *near,
        shared_gate,
        shared_up,
        shared_down,
        scratch=[
            pltpu.VMEM((inner_gate.shape[0] + 8, columns), F32),
            pltpu.VMEM((inner_gate.shape[0], columns), BF16),
            pltpu.VMEM((tp_count * row_count, width), BF16),
        ],
        limit=10,
    )

    parts = {}
    for g in reversed(range(groups)):
        done = on_core(
            functools.partial(combine_kernel, top, cap, tp_count, g, blocks),
            [VMEM] * (plane + 1),
            [((row_count, half), BF16, VMEM)] * (2 * blocks),
            *back,
            facts,
            scratch=[
                pltpu.VMEM((plane * blocks * cap, width), BF16),
                pltpu.VMEM((blocks * row_count, plane * blocks * cap), BF16),
                pltpu.VMEM((blocks * row_count, plane * blocks * cap), BF16),
            ],
            limit=10,
        )
        for b, n in enumerate(order[g * blocks : (g + 1) * blocks]):
            parts[n] = (done[2 * b], done[2 * b + 1])

    both, parts["u", reach] = lax.optimization_barrier((both, parts["u", reach]))
    total = both[0].astype(F32)
    for k in range(1, tp_count):
        total = total + lax.ppermute(both[k], "tp", ring(tp_count, k)).astype(F32)
    mixed_rows = rms_scale(total[:, :width], mixer_gain).astype(BF16)
    shared = total[:, width:]

    ends_a, ends_b = list(parts["u", reach]), list(parts["u", far])
    for s in range(reach - 1, -1, -1):
        for h in range(2):
            a = lax.ppermute(ends_a[h], "z", rise)
            ends_a[h] = a + parts["d", s][h] if s else a
            if s < far:
                b = lax.ppermute(ends_b[h], "z", fall)
                ends_b[h] = b + parts["u", s][h] if s else b
    sums = [
        ends_a[h].astype(F32) + ends_b[h].astype(F32) + parts["u", 0][h].astype(F32)
        for h in range(2)
    ]
    expert_rows = (shared + jnp.concatenate(sums, axis=1)).astype(BF16)
    return (mixed_rows, expert_rows)


def solution(mesh):
    sizes = dict(mesh.shape)
    sizes = (sizes["grp"], sizes["ep"] // CORES, CORES, sizes["tp"])
    fine = jax.sharding.Mesh(mesh.devices.reshape(sizes), ("grp", "z", "core", "tp"))
    sequence = P(("grp", "z", "core"), "tp")
    tokens = P(("grp", "z", "core", "tp"), None)
    experts = P(("z", "core", "tp"), None, None)
    return jax.shard_map(
        on_device,
        mesh=fine,
        in_specs=(
            sequence,
            sequence,
            sequence,
            P(),
            P("tp", None),
            P(),
            tokens,
            P(),
            tokens,
            tokens,
            experts,
            experts,
            experts,
            P(None, "tp"),
            P(None, "tp"),
            P("tp", None),
        ),
        out_specs=(tokens, tokens),
        check_vma=False,
    )
```

```python
import functools
import jax
import jax.numpy as jnp
from jax import lax
from jax.experimental import pallas as pl
from jax.experimental.pallas import tpu as pltpu
from jax.sharding import PartitionSpec as P

EPSILON = 1e-06
LANES = 128
CORES = 2
F32 = jnp.float32
BF16 = jnp.bfloat16
I32 = jnp.int32
MIB = 1024 * 1024
SIDE_STEP = 3
EXPERT_LIMIT = 50
VMEM = pl.BlockSpec(memory_space=pltpu.VMEM)
HBM = pl.BlockSpec(memory_space=pltpu.HBM)
AUTO = pl.BlockSpec()


def on_core(body, ins, outs, *args, scratch=(), limit=16):
    return pl.pallas_call(
        body,
        out_shape=[jax.ShapeDtypeStruct(s, t) for s, t, _ in outs],
        in_specs=ins,
        out_specs=[where for _, _, where in outs],
        scratch_shapes=list(scratch),
        compiler_params=pltpu.CompilerParams(vmem_limit_bytes=limit * MIB),
    )(*args)


def ring(size, by):
    return [(i, (i + by) % size) for i in range(size)]


def prepare_kernel(
    tokens, gain, ids, weights, inner_gate, inner_value, left, right, normed, last, arrived
):
    half = right.shape[1]
    tail = last.shape[0] // 2
    copies = [
        pltpu.make_async_copy(
            source.at[pl.ds(source.shape[0] - tail, tail), :],
            last.at[pl.ds(i * tail, tail), :],
            arrived.at[i],
        )
        for i, source in enumerate((inner_gate, inner_value))
    ]
    for copy in copies:
        copy.start()
    values = tokens[...].astype(F32)
    scale = lax.rsqrt(jnp.mean(values * values, axis=-1, keepdims=True) + EPSILON)
    rows = (values * scale * gain[...]).astype(BF16)
    normed[...] = rows
    left[:, :half] = rows[:, :half]
    right[...] = rows[:, half:]
    top, count = ids.shape
    most = weights[...].astype(BF16).astype(F32)
    lists = jnp.concatenate([ids[...].astype(F32), most, weights[...] - most], axis=0)
    above = lax.broadcasted_iota(I32, (count, count), 1)
    below = lax.broadcasted_iota(I32, (count, count), 0)
    same = (above == below).astype(F32).astype(BF16)
    turned = lax.dot_general(
        same, lists.astype(BF16), (((1,), (1,)), ((), ())), preferred_element_type=F32
    )
    lane = lax.broadcasted_iota(I32, (count, LANES), 1)
    named_ids = turned[:, :top].astype(I32)
    picks = [lane == named_ids[:, k : k + 1] for k in range(top)]
    named = functools.reduce(jnp.logical_or, picks).astype(F32).astype(BF16)
    before = (above < below).astype(F32).astype(BF16)
    seen = jnp.dot(before, named, preferred_element_type=F32)
    facts = jnp.zeros((count, LANES), F32)
    for k in range(top):
        rank = jnp.sum(jnp.where(picks[k], seen, 0.0), axis=1, keepdims=True)
        columns = (turned[:, k : k + 1], rank) + tuple(
            turned[:, i * top + k : i * top + k + 1] for i in (1, 2)
        )
        for place, value in enumerate(columns):
            facts = jnp.where(lane == place * top + k, value, facts)
    left[:, half:] = facts.astype(BF16)
    for copy in copies:
        copy.wait()


def slot_rows(facts, block, top, cap, per_place, tp_count):
    ids = facts[:, :top].astype(I32)
    ranks = facts[:, top : 2 * top].astype(I32)
    here = lax.axis_index("z") * CORES + lax.axis_index("core")
    at = ids // tp_count
    across = (at + here) % CORES
    along = (ids % tp_count - lax.axis_index("tp") + tp_count) % tp_count
    row = (across * tp_count + along) * per_place + block * cap + ranks
    return jnp.where(at // CORES == lax.axis_index("z"), row, -1)


def pick_kernel(top, cap, tp_count, groups, blocks, *refs):
    total, plane = groups * blocks, CORES * tp_count
    lefts, rights = refs[:total], refs[total : 2 * total]
    slots = refs[2 * total : 2 * total + plane]
    facts, held, chosen, arrived = refs[2 * total + plane :]
    count, half = rights[0].shape
    per_place = blocks * cap
    copies = []
    for b in range(total):
        span = pl.ds(b * count, count)
        copies.append(
            (
                pltpu.make_async_copy(
                    lefts[b].at[:, pl.ds(half, LANES)], facts.at[span, :], arrived.at[0, b]
                ),
                pltpu.make_async_copy(
                    lefts[b].at[:, pl.ds(0, half)], held.at[span, pl.ds(0, half)], arrived.at[1, b]
                ),
                pltpu.make_async_copy(
                    rights[b], held.at[span, pl.ds(half, half)], arrived.at[2, b]
                ),
            )
        )
    for trio in copies:
        for copy in trio:
            copy.start()
    wide = groups_lanes(plane * per_place)
    pair = LANES // count
    lane = lax.broadcasted_iota(I32, (count, wide), 1)
    for first in range(0, total, pair):
        hits = []
        for b in range(first, first + pair):
            copies[b][0].wait()
            known = facts[pl.ds(b * count, count), :].astype(F32)
            row = slot_rows(known, b % blocks, top, cap, per_place, tp_count)
            hit = functools.reduce(
                jnp.logical_or, [lane == row[:, k : k + 1] for k in range(top)]
            )
            hits.append(hit.astype(F32))
        turned = jnp.transpose(jnp.concatenate(hits, axis=0)).astype(BF16)
        g, at = first // blocks, first % blocks * count
        chosen[g, :, at : at + pair * count] = turned[: plane * per_place]
    for trio in copies:
        trio[1].wait()
        trio[2].wait()
    step = 512

    def columns(n, unused):
        span = pl.ds(pl.multiple_of(n * step, step), step)
        for g in range(groups):
            rows = held[pl.ds(g * blocks * count, blocks * count), span]
            got = jnp.dot(chosen[g], rows, preferred_element_type=F32).astype(BF16)
            for j in range(plane):
                slots[j][g * per_place : (g + 1) * per_place, span] = got[
                    j * per_place : (j + 1) * per_place
                ]
        return unused

    lax.fori_loop(0, 2 * half // step, columns, 0)


def groups_lanes(rows):
    return -(-rows // LANES) * LANES


def expert_kernel(plane, rows, *refs):
    pieces, sources = refs[:plane], refs[plane : plane + 3]
    outs = refs[plane + 3 : 2 * plane + 3]
    held, active, gate, up, down, arrived = refs[2 * plane + 3 :]
    copies = [
        pltpu.make_async_copy(source.at[0], target, arrived.at[i])
        for i, (source, target) in enumerate(zip(sources, (gate, up, down)))
    ]
    for copy in copies:
        copy.start()
    for j in range(plane):
        held[j * rows : (j + 1) * rows, :] = pieces[j][...]
    copies[0].wait()
    copies[1].wait()
    step = 256

    def hide(n, unused):
        span = pl.ds(pl.multiple_of(n * step, step), step)
        gate_value = jnp.dot(held[...], gate[:, span], preferred_element_type=F32)
        up_value = jnp.dot(held[...], up[:, span], preferred_element_type=F32)
        active[:, span] = (gate_value / (1.0 + jnp.exp(-gate_value)) * up_value).astype(BF16)
        return unused

    lax.fori_loop(0, gate.shape[1] // step, hide, 0)
    copies[2].wait()

    def show(n, unused):
        span = pl.ds(pl.multiple_of(n * step, step), step)
        got = jnp.dot(active[...], down[:, span], preferred_element_type=F32).astype(BF16)
        for j in range(plane):
            outs[j][:, span] = got[j * rows : (j + 1) * rows]
        return unused

    lax.fori_loop(0, down.shape[1] // step, show, 0)


def sides_kernel(tp_count, *refs):
    outer_gate, inner_gate, inner_value, before, taps, mixer_out = refs[:6]
    near, (gate, up, down) = refs[6 : 6 + tp_count], refs[6 + tp_count : 9 + tp_count]
    outs = refs[9 + tp_count : 9 + 2 * tp_count]
    product, scaled, held = refs[9 + 2 * tp_count :]
    rows, columns = inner_gate.shape
    count, width = near[0].shape
    tp = lax.axis_index("tp")
    halo = before.shape[0] // 2
    lead = product.shape[0] - rows
    earlier = before[...].astype(F32)
    product[lead - halo : lead, :] = earlier[:halo] * earlier[halo:]
    product[lead:, :] = inner_gate[...].astype(F32) * inner_value[...].astype(F32)
    tap = taps[:, pl.ds(pl.multiple_of(tp * columns, columns), columns)].astype(F32)
    filtered = tap[0:1] * product[lead - 2 : lead - 2 + rows, :]
    filtered = filtered + tap[1:2] * product[lead - 1 : lead - 1 + rows, :]
    filtered = filtered + tap[2:3] * product[lead : lead + rows, :]
    product[lead:, :] = outer_gate[...].astype(F32) * filtered
    for k in range(tp_count):
        at = pl.multiple_of((tp + k) % tp_count * count, count)
        scaled[k * count : (k + 1) * count, :] = product[pl.ds(lead + at, count), :].astype(BF16)
        held[k * count : (k + 1) * count, :] = near[-k % tp_count][...]
    gate_value = jnp.dot(held[...], gate[...], preferred_element_type=F32)
    up_value = jnp.dot(held[...], up[...], preferred_element_type=F32)
    active = (gate_value / (1.0 + jnp.exp(-gate_value)) * up_value).astype(BF16)
    step = 512

    def columns_of(n, unused):
        at = pl.multiple_of(n * step, step)
        mixed = jnp.dot(scaled[...], mixer_out[:, pl.ds(at, step)], preferred_element_type=F32)
        shared = jnp.dot(active, down[:, pl.ds(at, step)], preferred_element_type=F32)
        for k in range(tp_count):
            own = slice(k * count, (k + 1) * count)
            outs[k][:, pl.ds(at, step)] = mixed[own].astype(BF16)
            outs[k][:, pl.ds(width + at, step)] = shared[own].astype(BF16)
        return unused

    lax.fori_loop(0, width // step, columns_of, 0)


def combine_kernel(top, cap, tp_count, group, blocks, *refs):
    plane = CORES * tp_count
    back, facts = refs[:plane], refs[plane]
    outs = refs[plane + 1 : plane + 1 + 2 * blocks]
    held, high, low = refs[plane + 1 + 2 * blocks :]
    per_place = blocks * cap
    for j in range(plane):
        held[j * per_place : (j + 1) * per_place, :] = back[j][
            group * per_place : (group + 1) * per_place, :
        ]
    count, half = outs[0].shape
    lane = lax.broadcasted_iota(I32, (count, plane * per_place), 1)
    for b in range(blocks):
        known = facts[pl.ds((group * blocks + b) * count, count), :].astype(F32)
        row = slot_rows(known, b, top, cap, per_place, tp_count)
        most = jnp.zeros(lane.shape, F32)
        rest = jnp.zeros(lane.shape, F32)
        for k in range(top):
            hit = lane == row[:, k : k + 1]
            most = jnp.where(hit, known[:, 2 * top + k : 2 * top + k + 1], most)
            rest = jnp.where(hit, known[:, 3 * top + k : 3 * top + k + 1], rest)
        high[pl.ds(b * count, count), :] = most.astype(BF16)
        low[pl.ds(b * count, count), :] = rest.astype(BF16)
    step = 512
    for h in range(2):

        def columns(n, unused):
            at = pl.multiple_of(n * step, step)
            rows = held[:, pl.ds(h * half + at, step)]
            part = jnp.dot(high[...], rows, preferred_element_type=F32)
            part = part + jnp.dot(low[...], rows, preferred_element_type=F32)
            part = part.astype(BF16)
            for b in range(blocks):
                outs[2 * b + h][:, pl.ds(at, step)] = part[b * count : (b + 1) * count]
            return unused

        lax.fori_loop(0, half // step, columns, 0)


def plane_exchange(pieces, chips, tp_count):
    whole = [(z, core, i) for z in range(chips) for core in range(CORES) for i in range(tp_count)]

    def moved(piece, across, along):
        pairs = [
            (
                (z * CORES + core) * tp_count + i,
                (z * CORES + (core ^ across)) * tp_count + (i + along) % tp_count,
            )
            for z, core, i in whole
        ]
        return lax.ppermute(piece, ("z", "core", "tp"), pairs)

    middle = tp_count // 2
    halfway = [moved(pieces[middle], 0, 1), moved(pieces[tp_count + middle], 0, -1)]
    got = {0: pieces[0]}
    for along in (1, tp_count - 1):
        for across in range(CORES):
            got[across * tp_count + along] = moved(pieces[across * tp_count + along], across, along)
    got[tp_count] = moved(pieces[tp_count], 1, 0)
    got[middle] = moved(halfway[0], 0, middle - 1)
    got[tp_count + middle] = moved(halfway[1], 1, 1 - middle)
    return [got[j] for j in range(CORES * tp_count)]


def rms_scale(values, gains):
    return values * lax.rsqrt(jnp.mean(values * values, axis=-1, keepdims=True) + EPSILON) * gains


def on_device(
    outer_gate,
    inner_gate,
    inner_value,
    conv_taps,
    mixer_out,
    mixer_gain,
    moe_tokens,
    expert_gain,
    route_ids,
    route_weights,
    expert_gate,
    expert_up,
    expert_down,
    shared_gate,
    shared_up,
    shared_down,
):
    chips, tp_count = lax.axis_size("z"), lax.axis_size("tp")
    plane = CORES * tp_count
    tp = lax.axis_index("tp")
    row_count, width = moe_tokens.shape
    top = route_ids.shape[1]
    half = width // 2
    expert_count = chips * plane
    cap = (3 * row_count * top + 2 * expert_count - 1) // (2 * expert_count)
    reach = chips // 2
    far = chips - reach - 1

    left, right, normed, last = on_core(
        prepare_kernel,
        [AUTO] * 4 + [HBM] * 2,
        [
            ((row_count, half + LANES), BF16, VMEM),
            ((row_count, half), BF16, VMEM),
            ((row_count, width), BF16, VMEM),
            ((16, inner_gate.shape[1]), BF16, VMEM),
        ],
        moe_tokens,
        expert_gain.reshape(1, width),
        route_ids.T,
        route_weights.T,
        inner_gate,
        inner_value,
        scratch=[pltpu.SemaphoreType.DMA((2,))],
        limit=56,
    )

    near = [normed] + [lax.ppermute(normed, "tp", ring(tp_count, k)) for k in range(1, tp_count)]
    pairs = [(i, i + 1) for i in range(chips * CORES - 1)]
    before = lax.ppermute(last, ("z", "core"), pairs)

    rise, fall = ring(chips, 1), ring(chips, -1)
    got = {("u", 0): (left, right), ("d", 0): (left, right)}
    order = [("u", 0)]
    for s in range(1, reach + 1):
        if s == SIDE_STEP:
            near, before, got["u", s - 1] = lax.optimization_barrier(
                (near, before, got["u", s - 1])
            )
        got["u", s] = tuple(lax.ppermute(v, "z", rise) for v in got["u", s - 1])
        order.append(("u", s))
        if s <= far:
            got["d", s] = tuple(lax.ppermute(v, "z", fall) for v in got["d", s - 1])
            order.append(("d", s))

    groups = 2
    blocks = chips // groups
    rows = chips * cap
    lefts = [got[n][0] for n in order]
    rights = [got[n][1] for n in order]
    *slots, facts = on_core(
        functools.partial(pick_kernel, top, cap, tp_count, groups, blocks),
        [HBM] * (2 * chips),
        [((rows, width), BF16, VMEM)] * plane + [((chips * row_count, LANES), BF16, VMEM)],
        *lefts,
        *rights,
        scratch=[
            pltpu.VMEM((chips * row_count, width), BF16),
            pltpu.VMEM((groups, plane * blocks * cap, blocks * row_count), BF16),
            pltpu.SemaphoreType.DMA((3, chips)),
        ],
        limit=12,
    )
    here = plane_exchange(slots, chips, tp_count)
    hidden = expert_gate.shape[2]
    result = on_core(
        functools.partial(expert_kernel, plane, rows),
        [VMEM] * plane + [HBM] * 3,
        [((rows, width), BF16, VMEM)] * plane,
        *here,
        expert_gate,
        expert_up,
        expert_down,
        scratch=[
            pltpu.VMEM((plane * rows, width), BF16),
            pltpu.VMEM((plane * rows, hidden), BF16),
            pltpu.VMEM((width, hidden), BF16),
            pltpu.VMEM((width, hidden), BF16),
            pltpu.VMEM((hidden, width), BF16),
            pltpu.SemaphoreType.DMA((3,)),
        ],
        limit=EXPERT_LIMIT,
    )
    turned = [result[a * tp_count + -k % tp_count] for a in range(CORES) for k in range(tp_count)]
    turned = plane_exchange(turned, chips, tp_count)
    back = [turned[a * tp_count + -k % tp_count] for a in range(CORES) for k in range(tp_count)]

    columns = inner_gate.shape[1]
    both = on_core(
        functools.partial(sides_kernel, tp_count),
        [VMEM] * (9 + tp_count),
        [((row_count, 2 * width), BF16, VMEM)] * tp_count,
        outer_gate,
        inner_gate,
        inner_value,
        before,
        conv_taps,
        mixer_out,
        *near,
        shared_gate,
        shared_up,
        shared_down,
        scratch=[
            pltpu.VMEM((inner_gate.shape[0] + 8, columns), F32),
            pltpu.VMEM((inner_gate.shape[0], columns), BF16),
            pltpu.VMEM((tp_count * row_count, width), BF16),
        ],
        limit=10,
    )

    parts = {}
    for g in reversed(range(groups)):
        done = on_core(
            functools.partial(combine_kernel, top, cap, tp_count, g, blocks),
            [VMEM] * (plane + 1),
            [((row_count, half), BF16, VMEM)] * (2 * blocks),
            *back,
            facts,
            scratch=[
                pltpu.VMEM((plane * blocks * cap, width), BF16),
                pltpu.VMEM((blocks * row_count, plane * blocks * cap), BF16),
                pltpu.VMEM((blocks * row_count, plane * blocks * cap), BF16),
            ],
            limit=10,
        )
        for b, n in enumerate(order[g * blocks : (g + 1) * blocks]):
            parts[n] = (done[2 * b], done[2 * b + 1])

    both, parts["u", reach] = lax.optimization_barrier((both, parts["u", reach]))
    total = both[0].astype(F32)
    for k in range(1, tp_count):
        total = total + lax.ppermute(both[k], "tp", ring(tp_count, k)).astype(F32)
    mixed_rows = rms_scale(total[:, :width], mixer_gain).astype(BF16)
    shared = total[:, width:]

    ends_a, ends_b = list(parts["u", reach]), list(parts["u", far])
    for s in range(reach - 1, -1, -1):
        for h in range(2):
            a = lax.ppermute(ends_a[h], "z", rise)
            ends_a[h] = a + parts["d", s][h] if s else a
            if s < far:
                b = lax.ppermute(ends_b[h], "z", fall)
                ends_b[h] = b + parts["u", s][h] if s else b
    sums = [
        ends_a[h].astype(F32) + ends_b[h].astype(F32) + parts["u", 0][h].astype(F32)
        for h in range(2)
    ]
    expert_rows = (shared + jnp.concatenate(sums, axis=1)).astype(BF16)
    return (mixed_rows, expert_rows)


def solution(mesh):
    sizes = dict(mesh.shape)
    sizes = (sizes["grp"], sizes["ep"] // CORES, CORES, sizes["tp"])
    fine = jax.sharding.Mesh(mesh.devices.reshape(sizes), ("grp", "z", "core", "tp"))
    sequence = P(("grp", "z", "core"), "tp")
    tokens = P(("grp", "z", "core", "tp"), None)
    experts = P(("z", "core", "tp"), None, None)
    return jax.shard_map(
        on_device,
        mesh=fine,
        in_specs=(
            sequence,
            sequence,
            sequence,
            P(),
            P("tp", None),
            P(),
            tokens,
            P(),
            tokens,
            tokens,
            experts,
            experts,
            experts,
            P(None, "tp"),
            P(None, "tp"),
            P("tp", None),
        ),
        out_specs=(tokens, tokens),
        check_vma=False,
    )
```

```python
import functools
import jax
import jax.numpy as jnp
from jax import lax
from jax.experimental import pallas as pl
from jax.experimental.pallas import tpu as pltpu
from jax.sharding import PartitionSpec as P

EPSILON = 1e-06
LANES = 128
CORES = 2
F32 = jnp.float32
BF16 = jnp.bfloat16
I32 = jnp.int32
MIB = 1024 * 1024
SIDE_STEP = 3
EXCHANGE_STEP = 0
EXPERT_LIMIT = 50
VMEM = pl.BlockSpec(memory_space=pltpu.VMEM)
HBM = pl.BlockSpec(memory_space=pltpu.HBM)
AUTO = pl.BlockSpec()


def on_core(body, ins, outs, *args, scratch=(), limit=16):
    return pl.pallas_call(
        body,
        out_shape=[jax.ShapeDtypeStruct(s, t) for s, t, _ in outs],
        in_specs=ins,
        out_specs=[where for _, _, where in outs],
        scratch_shapes=list(scratch),
        compiler_params=pltpu.CompilerParams(vmem_limit_bytes=limit * MIB),
    )(*args)


def ring(size, by):
    return [(i, (i + by) % size) for i in range(size)]


def prepare_kernel(
    tokens, gain, ids, weights, inner_gate, inner_value, left, right, normed, last, arrived
):
    half = right.shape[1]
    tail = last.shape[0] // 2
    copies = [
        pltpu.make_async_copy(
            source.at[pl.ds(source.shape[0] - tail, tail), :],
            last.at[pl.ds(i * tail, tail), :],
            arrived.at[i],
        )
        for i, source in enumerate((inner_gate, inner_value))
    ]
    for copy in copies:
        copy.start()
    values = tokens[...].astype(F32)
    scale = lax.rsqrt(jnp.mean(values * values, axis=-1, keepdims=True) + EPSILON)
    rows = (values * scale * gain[...]).astype(BF16)
    normed[...] = rows
    left[:, :half] = rows[:, :half]
    right[...] = rows[:, half:]
    top, count = ids.shape
    most = weights[...].astype(BF16).astype(F32)
    lists = jnp.concatenate([ids[...].astype(F32), most, weights[...] - most], axis=0)
    above = lax.broadcasted_iota(I32, (count, count), 1)
    below = lax.broadcasted_iota(I32, (count, count), 0)
    same = (above == below).astype(F32).astype(BF16)
    turned = lax.dot_general(
        same, lists.astype(BF16), (((1,), (1,)), ((), ())), preferred_element_type=F32
    )
    lane = lax.broadcasted_iota(I32, (count, LANES), 1)
    named_ids = turned[:, :top].astype(I32)
    picks = [lane == named_ids[:, k : k + 1] for k in range(top)]
    named = functools.reduce(jnp.logical_or, picks).astype(F32).astype(BF16)
    before = (above < below).astype(F32).astype(BF16)
    seen = jnp.dot(before, named, preferred_element_type=F32)
    facts = jnp.zeros((count, LANES), F32)
    for k in range(top):
        rank = jnp.sum(jnp.where(picks[k], seen, 0.0), axis=1, keepdims=True)
        columns = (turned[:, k : k + 1], rank) + tuple(
            turned[:, i * top + k : i * top + k + 1] for i in (1, 2)
        )
        for place, value in enumerate(columns):
            facts = jnp.where(lane == place * top + k, value, facts)
    left[:, half:] = facts.astype(BF16)
    for copy in copies:
        copy.wait()


def slot_rows(facts, block, top, cap, per_place, tp_count):
    ids = facts[:, :top].astype(I32)
    ranks = facts[:, top : 2 * top].astype(I32)
    here = lax.axis_index("z") * CORES + lax.axis_index("core")
    at = ids // tp_count
    across = (at + here) % CORES
    along = (ids % tp_count - lax.axis_index("tp") + tp_count) % tp_count
    row = (across * tp_count + along) * per_place + block * cap + ranks
    return jnp.where(at // CORES == lax.axis_index("z"), row, -1)


def pick_kernel(top, cap, tp_count, groups, blocks, *refs):
    total, plane = groups * blocks, CORES * tp_count
    lefts, rights = refs[:total], refs[total : 2 * total]
    slots = refs[2 * total : 2 * total + plane]
    facts, held, chosen = refs[2 * total + plane :]
    count, half = rights[0].shape
    per_place = blocks * cap
    wide = groups_lanes(plane * per_place)
    pair = LANES // count
    lane = lax.broadcasted_iota(I32, (count, wide), 1)
    for first in range(0, total, pair):
        hits = []
        for b in range(first, first + pair):
            own = slice(b * count, (b + 1) * count)
            held[own, :half] = lefts[b][:, :half]
            held[own, half:] = rights[b][...]
            facts[own, :] = lefts[b][:, half:]
            known = lefts[b][:, half:].astype(F32)
            row = slot_rows(known, b % blocks, top, cap, per_place, tp_count)
            hit = functools.reduce(
                jnp.logical_or, [lane == row[:, k : k + 1] for k in range(top)]
            )
            hits.append(hit.astype(F32))
        turned = jnp.transpose(jnp.concatenate(hits, axis=0)).astype(BF16)
        g, at = first // blocks, first % blocks * count
        chosen[g, :, at : at + pair * count] = turned[: plane * per_place]
    step = 512

    def columns(n, unused):
        span = pl.ds(pl.multiple_of(n * step, step), step)
        for g in range(groups):
            rows = held[pl.ds(g * blocks * count, blocks * count), span]
            got = jnp.dot(chosen[g], rows, preferred_element_type=F32).astype(BF16)
            for j in range(plane):
                slots[j][g * per_place : (g + 1) * per_place, span] = got[
                    j * per_place : (j + 1) * per_place
                ]
        return unused

    lax.fori_loop(0, 2 * half // step, columns, 0)


def groups_lanes(rows):
    return -(-rows // LANES) * LANES


def expert_kernel(plane, rows, *refs):
    pieces, sources = refs[:plane], refs[plane : plane + 3]
    outs = refs[plane + 3 : 2 * plane + 3]
    held, active, gate, up, down, arrived = refs[2 * plane + 3 :]
    copies = [
        pltpu.make_async_copy(source.at[0], target, arrived.at[i])
        for i, (source, target) in enumerate(zip(sources, (gate, up, down)))
    ]
    for copy in copies:
        copy.start()
    for j in range(plane):
        held[j * rows : (j + 1) * rows, :] = pieces[j][...]
    copies[0].wait()
    copies[1].wait()
    step = 256

    def hide(n, unused):
        span = pl.ds(pl.multiple_of(n * step, step), step)
        gate_value = jnp.dot(held[...], gate[:, span], preferred_element_type=F32)
        up_value = jnp.dot(held[...], up[:, span], preferred_element_type=F32)
        active[:, span] = (gate_value / (1.0 + jnp.exp(-gate_value)) * up_value).astype(BF16)
        return unused

    lax.fori_loop(0, gate.shape[1] // step, hide, 0)
    copies[2].wait()

    def show(n, unused):
        span = pl.ds(pl.multiple_of(n * step, step), step)
        got = jnp.dot(active[...], down[:, span], preferred_element_type=F32).astype(BF16)
        for j in range(plane):
            outs[j][:, span] = got[j * rows : (j + 1) * rows]
        return unused

    lax.fori_loop(0, down.shape[1] // step, show, 0)


def sides_kernel(tp_count, *refs):
    outer_gate, inner_gate, inner_value, before, taps, mixer_out = refs[:6]
    near, (gate, up, down) = refs[6 : 6 + tp_count], refs[6 + tp_count : 9 + tp_count]
    outs = refs[9 + tp_count : 9 + 2 * tp_count]
    product, scaled, held = refs[9 + 2 * tp_count :]
    rows, columns = inner_gate.shape
    count, width = near[0].shape
    tp = lax.axis_index("tp")
    halo = before.shape[0] // 2
    lead = product.shape[0] - rows
    earlier = before[...].astype(F32)
    product[lead - halo : lead, :] = earlier[:halo] * earlier[halo:]
    product[lead:, :] = inner_gate[...].astype(F32) * inner_value[...].astype(F32)
    tap = taps[:, pl.ds(pl.multiple_of(tp * columns, columns), columns)].astype(F32)
    filtered = tap[0:1] * product[lead - 2 : lead - 2 + rows, :]
    filtered = filtered + tap[1:2] * product[lead - 1 : lead - 1 + rows, :]
    filtered = filtered + tap[2:3] * product[lead : lead + rows, :]
    product[lead:, :] = outer_gate[...].astype(F32) * filtered
    for k in range(tp_count):
        at = pl.multiple_of((tp + k) % tp_count * count, count)
        scaled[k * count : (k + 1) * count, :] = product[pl.ds(lead + at, count), :].astype(BF16)
        held[k * count : (k + 1) * count, :] = near[-k % tp_count][...]
    gate_value = jnp.dot(held[...], gate[...], preferred_element_type=F32)
    up_value = jnp.dot(held[...], up[...], preferred_element_type=F32)
    active = (gate_value / (1.0 + jnp.exp(-gate_value)) * up_value).astype(BF16)
    step = 512

    def columns_of(n, unused):
        at = pl.multiple_of(n * step, step)
        mixed = jnp.dot(scaled[...], mixer_out[:, pl.ds(at, step)], preferred_element_type=F32)
        shared = jnp.dot(active, down[:, pl.ds(at, step)], preferred_element_type=F32)
        for k in range(tp_count):
            own = slice(k * count, (k + 1) * count)
            outs[k][:, pl.ds(at, step)] = mixed[own].astype(BF16)
            outs[k][:, pl.ds(width + at, step)] = shared[own].astype(BF16)
        return unused

    lax.fori_loop(0, width // step, columns_of, 0)


def combine_kernel(top, cap, tp_count, group, blocks, *refs):
    plane = CORES * tp_count
    back, facts = refs[:plane], refs[plane]
    outs = refs[plane + 1 : plane + 1 + 2 * blocks]
    held, high, low = refs[plane + 1 + 2 * blocks :]
    per_place = blocks * cap
    for j in range(plane):
        held[j * per_place : (j + 1) * per_place, :] = back[j][
            group * per_place : (group + 1) * per_place, :
        ]
    count, half = outs[0].shape
    lane = lax.broadcasted_iota(I32, (count, plane * per_place), 1)
    for b in range(blocks):
        known = facts[pl.ds((group * blocks + b) * count, count), :].astype(F32)
        row = slot_rows(known, b, top, cap, per_place, tp_count)
        most = jnp.zeros(lane.shape, F32)
        rest = jnp.zeros(lane.shape, F32)
        for k in range(top):
            hit = lane == row[:, k : k + 1]
            most = jnp.where(hit, known[:, 2 * top + k : 2 * top + k + 1], most)
            rest = jnp.where(hit, known[:, 3 * top + k : 3 * top + k + 1], rest)
        high[pl.ds(b * count, count), :] = most.astype(BF16)
        low[pl.ds(b * count, count), :] = rest.astype(BF16)
    step = 512
    for h in range(2):

        def columns(n, unused):
            at = pl.multiple_of(n * step, step)
            rows = held[:, pl.ds(h * half + at, step)]
            part = jnp.dot(high[...], rows, preferred_element_type=F32)
            part = part + jnp.dot(low[...], rows, preferred_element_type=F32)
            part = part.astype(BF16)
            for b in range(blocks):
                outs[2 * b + h][:, pl.ds(at, step)] = part[b * count : (b + 1) * count]
            return unused

        lax.fori_loop(0, half // step, columns, 0)


def plane_exchange(pieces, chips, tp_count):
    whole = [(z, core, i) for z in range(chips) for core in range(CORES) for i in range(tp_count)]

    def moved(piece, across, along):
        pairs = [
            (
                (z * CORES + core) * tp_count + i,
                (z * CORES + (core ^ across)) * tp_count + (i + along) % tp_count,
            )
            for z, core, i in whole
        ]
        return lax.ppermute(piece, ("z", "core", "tp"), pairs)

    middle = tp_count // 2
    halfway = [moved(pieces[middle], 0, 1), moved(pieces[tp_count + middle], 0, -1)]
    got = {0: pieces[0]}
    for along in (1, tp_count - 1):
        for across in range(CORES):
            got[across * tp_count + along] = moved(pieces[across * tp_count + along], across, along)
    got[tp_count] = moved(pieces[tp_count], 1, 0)
    got[middle] = moved(halfway[0], 0, middle - 1)
    got[tp_count + middle] = moved(halfway[1], 1, 1 - middle)
    return [got[j] for j in range(CORES * tp_count)]


def rms_scale(values, gains):
    return values * lax.rsqrt(jnp.mean(values * values, axis=-1, keepdims=True) + EPSILON) * gains


def on_device(
    outer_gate,
    inner_gate,
    inner_value,
    conv_taps,
    mixer_out,
    mixer_gain,
    moe_tokens,
    expert_gain,
    route_ids,
    route_weights,
    expert_gate,
    expert_up,
    expert_down,
    shared_gate,
    shared_up,
    shared_down,
):
    chips, tp_count = lax.axis_size("z"), lax.axis_size("tp")
    plane = CORES * tp_count
    tp = lax.axis_index("tp")
    row_count, width = moe_tokens.shape
    top = route_ids.shape[1]
    half = width // 2
    expert_count = chips * plane
    cap = (3 * row_count * top + 2 * expert_count - 1) // (2 * expert_count)
    reach = chips // 2
    far = chips - reach - 1

    left, right, normed, last = on_core(
        prepare_kernel,
        [AUTO] * 4 + [HBM] * 2,
        [
            ((row_count, half + LANES), BF16, VMEM),
            ((row_count, half), BF16, VMEM),
            ((row_count, width), BF16, VMEM),
            ((16, inner_gate.shape[1]), BF16, VMEM),
        ],
        moe_tokens,
        expert_gain.reshape(1, width),
        route_ids.T,
        route_weights.T,
        inner_gate,
        inner_value,
        scratch=[pltpu.SemaphoreType.DMA((2,))],
        limit=56,
    )

    near = [normed] + [lax.ppermute(normed, "tp", ring(tp_count, k)) for k in range(1, tp_count)]
    pairs = [(i, i + 1) for i in range(chips * CORES - 1)]
    before = lax.ppermute(last, ("z", "core"), pairs)

    rise, fall = ring(chips, 1), ring(chips, -1)
    got = {("u", 0): (left, right), ("d", 0): (left, right)}
    order = [("u", 0)]
    for s in range(1, far + 1):
        if s == SIDE_STEP:
            near, before, got["u", s - 1] = lax.optimization_barrier(
                (near, before, got["u", s - 1])
            )
        got["u", s] = tuple(lax.ppermute(v, "z", rise) for v in got["u", s - 1])
        got["d", s] = tuple(lax.ppermute(v, "z", fall) for v in got["d", s - 1])
        order += [("u", s), ("d", s)]
    got["u", reach] = (
        lax.ppermute(got["u", far][0], "z", rise),
        lax.ppermute(got["d", far][1], "z", fall),
    )
    order.append(("u", reach))

    groups = 2
    blocks = chips // groups
    rows = chips * cap
    lefts = [got[n][0] for n in order]
    rights = [got[n][1] for n in order]
    *slots, facts = on_core(
        functools.partial(pick_kernel, top, cap, tp_count, groups, blocks),
        [VMEM] * (2 * chips),
        [((rows, width), BF16, VMEM)] * plane + [((chips * row_count, LANES), BF16, VMEM)],
        *lefts,
        *rights,
        scratch=[
            pltpu.VMEM((chips * row_count, width), BF16),
            pltpu.VMEM((groups, plane * blocks * cap, blocks * row_count), BF16),
        ],
        limit=12,
    )
    here = plane_exchange(slots, chips, tp_count)
    hidden = expert_gate.shape[2]
    result = on_core(
        functools.partial(expert_kernel, plane, rows),
        [VMEM] * plane + [HBM] * 3,
        [((rows, width), BF16, VMEM)] * plane,
        *here,
        expert_gate,
        expert_up,
        expert_down,
        scratch=[
            pltpu.VMEM((plane * rows, width), BF16),
            pltpu.VMEM((plane * rows, hidden), BF16),
            pltpu.VMEM((width, hidden), BF16),
            pltpu.VMEM((width, hidden), BF16),
            pltpu.VMEM((hidden, width), BF16),
            pltpu.SemaphoreType.DMA((3,)),
        ],
        limit=EXPERT_LIMIT,
    )
    turned = [result[a * tp_count + -k % tp_count] for a in range(CORES) for k in range(tp_count)]
    turned = plane_exchange(turned, chips, tp_count)
    back = [turned[a * tp_count + -k % tp_count] for a in range(CORES) for k in range(tp_count)]

    columns = inner_gate.shape[1]
    both = on_core(
        functools.partial(sides_kernel, tp_count),
        [VMEM] * (9 + tp_count),
        [((row_count, 2 * width), BF16, VMEM)] * tp_count,
        outer_gate,
        inner_gate,
        inner_value,
        before,
        conv_taps,
        mixer_out,
        *near,
        shared_gate,
        shared_up,
        shared_down,
        scratch=[
            pltpu.VMEM((inner_gate.shape[0] + 8, columns), F32),
            pltpu.VMEM((inner_gate.shape[0], columns), BF16),
            pltpu.VMEM((tp_count * row_count, width), BF16),
        ],
        limit=10,
    )

    both, back = lax.optimization_barrier((list(both), back))
    parts = {}
    for g in reversed(range(groups)):
        done = on_core(
            functools.partial(combine_kernel, top, cap, tp_count, g, blocks),
            [VMEM] * (plane + 1),
            [((row_count, half), BF16, VMEM)] * (2 * blocks),
            *back,
            facts,
            scratch=[
                pltpu.VMEM((plane * blocks * cap, width), BF16),
                pltpu.VMEM((blocks * row_count, plane * blocks * cap), BF16),
                pltpu.VMEM((blocks * row_count, plane * blocks * cap), BF16),
            ],
            limit=10,
        )
        for b, n in enumerate(order[g * blocks : (g + 1) * blocks]):
            parts[n] = (done[2 * b], done[2 * b + 1])

    total = both[0].astype(F32)
    rising = [parts["u", reach][0], parts["d", far][1]]
    falling = [parts["u", far][0], parts["u", reach][1]]
    for s in range(reach, 0, -1):
        for h in range(2):
            first_up, first_down = (reach, far) if h == 0 else (far, reach)
            if s <= first_up:
                rising[h] = lax.ppermute(rising[h], "z", rise)
                if s > 1:
                    rising[h] = rising[h] + parts["d", s - 1][h]
            if s <= first_down:
                falling[h] = lax.ppermute(falling[h], "z", fall)
                if s > 1:
                    falling[h] = falling[h] + parts["u", s - 1][h]
        k = reach - EXCHANGE_STEP - s
        if 1 <= k < tp_count:
            both[k], rising[0] = lax.optimization_barrier((both[k], rising[0]))
            total = total + lax.ppermute(both[k], "tp", ring(tp_count, k)).astype(F32)
    sums = [
        rising[h].astype(F32) + falling[h].astype(F32) + parts["u", 0][h].astype(F32)
        for h in range(2)
    ]
    mixed_rows = rms_scale(total[:, :width], mixer_gain).astype(BF16)
    shared = total[:, width:]
    expert_rows = (shared + jnp.concatenate(sums, axis=1)).astype(BF16)
    return (mixed_rows, expert_rows)


def solution(mesh):
    sizes = dict(mesh.shape)
    sizes = (sizes["grp"], sizes["ep"] // CORES, CORES, sizes["tp"])
    fine = jax.sharding.Mesh(mesh.devices.reshape(sizes), ("grp", "z", "core", "tp"))
    sequence = P(("grp", "z", "core"), "tp")
    tokens = P(("grp", "z", "core", "tp"), None)
    experts = P(("z", "core", "tp"), None, None)
    return jax.shard_map(
        on_device,
        mesh=fine,
        in_specs=(
            sequence,
            sequence,
            sequence,
            P(),
            P("tp", None),
            P(),
            tokens,
            P(),
            tokens,
            tokens,
            experts,
            experts,
            experts,
            P(None, "tp"),
            P(None, "tp"),
            P("tp", None),
        ),
        out_specs=(tokens, tokens),
        check_vma=False,
    )
```

```python
import functools
import jax
import jax.numpy as jnp
from jax import lax
from jax.experimental import pallas as pl
from jax.experimental.pallas import tpu as pltpu
from jax.sharding import PartitionSpec as P

EPSILON = 1e-06
LANES = 128
CORES = 2
F32 = jnp.float32
BF16 = jnp.bfloat16
I32 = jnp.int32
MIB = 1024 * 1024
SIDE_STEP = 3
EXCHANGE_STEP = 0
EXPERT_LIMIT = 50
VMEM = pl.BlockSpec(memory_space=pltpu.VMEM)
HBM = pl.BlockSpec(memory_space=pltpu.HBM)
AUTO = pl.BlockSpec()


def on_core(body, ins, outs, *args, scratch=(), limit=16):
    return pl.pallas_call(
        body,
        out_shape=[jax.ShapeDtypeStruct(s, t) for s, t, _ in outs],
        in_specs=ins,
        out_specs=[where for _, _, where in outs],
        scratch_shapes=list(scratch),
        compiler_params=pltpu.CompilerParams(vmem_limit_bytes=limit * MIB),
    )(*args)


def ring(size, by):
    return [(i, (i + by) % size) for i in range(size)]


def prepare_kernel(
    tokens, gain, ids, weights, inner_gate, inner_value, left, right, normed, last, arrived
):
    half = right.shape[1]
    tail = last.shape[0] // 2
    copies = [
        pltpu.make_async_copy(
            source.at[pl.ds(source.shape[0] - tail, tail), :],
            last.at[pl.ds(i * tail, tail), :],
            arrived.at[i],
        )
        for i, source in enumerate((inner_gate, inner_value))
    ]
    for copy in copies:
        copy.start()
    values = tokens[...].astype(F32)
    scale = lax.rsqrt(jnp.mean(values * values, axis=-1, keepdims=True) + EPSILON)
    rows = (values * scale * gain[...]).astype(BF16)
    normed[...] = rows
    left[:, :half] = rows[:, :half]
    right[...] = rows[:, half:]
    top, count = ids.shape
    most = weights[...].astype(BF16).astype(F32)
    lists = jnp.concatenate([ids[...].astype(F32), most, weights[...] - most], axis=0)
    above = lax.broadcasted_iota(I32, (count, count), 1)
    below = lax.broadcasted_iota(I32, (count, count), 0)
    same = (above == below).astype(F32).astype(BF16)
    turned = lax.dot_general(
        same, lists.astype(BF16), (((1,), (1,)), ((), ())), preferred_element_type=F32
    )
    lane = lax.broadcasted_iota(I32, (count, LANES), 1)
    named_ids = turned[:, :top].astype(I32)
    picks = [lane == named_ids[:, k : k + 1] for k in range(top)]
    named = functools.reduce(jnp.logical_or, picks).astype(F32).astype(BF16)
    before = (above < below).astype(F32).astype(BF16)
    seen = jnp.dot(before, named, preferred_element_type=F32)
    facts = jnp.zeros((count, LANES), F32)
    for k in range(top):
        rank = jnp.sum(jnp.where(picks[k], seen, 0.0), axis=1, keepdims=True)
        columns = (turned[:, k : k + 1], rank) + tuple(
            turned[:, i * top + k : i * top + k + 1] for i in (1, 2)
        )
        for place, value in enumerate(columns):
            facts = jnp.where(lane == place * top + k, value, facts)
    left[:, half:] = facts.astype(BF16)
    for copy in copies:
        copy.wait()


def slot_rows(facts, block, top, cap, per_place, tp_count):
    ids = facts[:, :top].astype(I32)
    ranks = facts[:, top : 2 * top].astype(I32)
    here = lax.axis_index("z") * CORES + lax.axis_index("core")
    at = ids // tp_count
    across = (at + here) % CORES
    along = (ids % tp_count - lax.axis_index("tp") + tp_count) % tp_count
    row = (across * tp_count + along) * per_place + block * cap + ranks
    return jnp.where(at // CORES == lax.axis_index("z"), row, -1)


def pick_kernel(top, cap, tp_count, groups, blocks, *refs):
    total, plane = groups * blocks, CORES * tp_count
    lefts, rights = refs[:total], refs[total : 2 * total]
    slots = refs[2 * total : 2 * total + plane]
    facts, held, chosen = refs[2 * total + plane :]
    count, half = rights[0].shape
    per_place = blocks * cap
    wide = groups_lanes(plane * per_place)
    pair = LANES // count
    lane = lax.broadcasted_iota(I32, (count, wide), 1)
    for first in range(0, total, pair):
        hits = []
        for b in range(first, first + pair):
            own = slice(b * count, (b + 1) * count)
            held[own, :half] = lefts[b][:, :half]
            held[own, half:] = rights[b][...]
            facts[own, :] = lefts[b][:, half:]
            known = lefts[b][:, half:].astype(F32)
            row = slot_rows(known, b % blocks, top, cap, per_place, tp_count)
            hit = functools.reduce(
                jnp.logical_or, [lane == row[:, k : k + 1] for k in range(top)]
            )
            hits.append(hit.astype(F32))
        turned = jnp.transpose(jnp.concatenate(hits, axis=0)).astype(BF16)
        g, at = first // blocks, first % blocks * count
        chosen[g, :, at : at + pair * count] = turned[: plane * per_place]
    step = 512

    def columns(n, unused):
        span = pl.ds(pl.multiple_of(n * step, step), step)
        for g in range(groups):
            rows = held[pl.ds(g * blocks * count, blocks * count), span]
            got = jnp.dot(chosen[g], rows, preferred_element_type=F32).astype(BF16)
            for j in range(plane):
                slots[j][g * per_place : (g + 1) * per_place, span] = got[
                    j * per_place : (j + 1) * per_place
                ]
        return unused

    lax.fori_loop(0, 2 * half // step, columns, 0)


def groups_lanes(rows):
    return -(-rows // LANES) * LANES


def expert_kernel(plane, rows, *refs):
    pieces, sources = refs[:plane], refs[plane : plane + 3]
    outs = refs[plane + 3 : 2 * plane + 3]
    held, active, gate, up, down, arrived = refs[2 * plane + 3 :]
    copies = [
        pltpu.make_async_copy(source.at[0], target, arrived.at[i])
        for i, (source, target) in enumerate(zip(sources, (gate, up, down)))
    ]
    for copy in copies:
        copy.start()
    for j in range(plane):
        held[j * rows : (j + 1) * rows, :] = pieces[j][...]
    copies[0].wait()
    copies[1].wait()
    step = 256

    def hide(n, unused):
        span = pl.ds(pl.multiple_of(n * step, step), step)
        gate_value = jnp.dot(held[...], gate[:, span], preferred_element_type=F32)
        up_value = jnp.dot(held[...], up[:, span], preferred_element_type=F32)
        active[:, span] = (gate_value / (1.0 + jnp.exp(-gate_value)) * up_value).astype(BF16)
        return unused

    lax.fori_loop(0, gate.shape[1] // step, hide, 0)
    copies[2].wait()

    def show(n, unused):
        span = pl.ds(pl.multiple_of(n * step, step), step)
        got = jnp.dot(active[...], down[:, span], preferred_element_type=F32).astype(BF16)
        for j in range(plane):
            outs[j][:, span] = got[j * rows : (j + 1) * rows]
        return unused

    lax.fori_loop(0, down.shape[1] // step, show, 0)


def sides_kernel(tp_count, *refs):
    outer_gate, inner_gate, inner_value, before, taps, mixer_out = refs[:6]
    near, (gate, up, down) = refs[6 : 6 + tp_count], refs[6 + tp_count : 9 + tp_count]
    outs = refs[9 + tp_count : 9 + 2 * tp_count]
    product, scaled, held = refs[9 + 2 * tp_count :]
    rows, columns = inner_gate.shape
    count, width = near[0].shape
    tp = lax.axis_index("tp")
    halo = before.shape[0] // 2
    lead = product.shape[0] - rows
    earlier = before[...].astype(F32)
    product[lead - halo : lead, :] = earlier[:halo] * earlier[halo:]
    product[lead:, :] = inner_gate[...].astype(F32) * inner_value[...].astype(F32)
    tap = taps[:, pl.ds(pl.multiple_of(tp * columns, columns), columns)].astype(F32)
    filtered = tap[0:1] * product[lead - 2 : lead - 2 + rows, :]
    filtered = filtered + tap[1:2] * product[lead - 1 : lead - 1 + rows, :]
    filtered = filtered + tap[2:3] * product[lead : lead + rows, :]
    product[lead:, :] = outer_gate[...].astype(F32) * filtered
    for k in range(tp_count):
        at = pl.multiple_of((tp + k) % tp_count * count, count)
        scaled[k * count : (k + 1) * count, :] = product[pl.ds(lead + at, count), :].astype(BF16)
        held[k * count : (k + 1) * count, :] = near[-k % tp_count][...]
    gate_value = jnp.dot(held[...], gate[...], preferred_element_type=F32)
    up_value = jnp.dot(held[...], up[...], preferred_element_type=F32)
    active = (gate_value / (1.0 + jnp.exp(-gate_value)) * up_value).astype(BF16)
    step = 512

    def columns_of(n, unused):
        at = pl.multiple_of(n * step, step)
        mixed = jnp.dot(scaled[...], mixer_out[:, pl.ds(at, step)], preferred_element_type=F32)
        shared = jnp.dot(active, down[:, pl.ds(at, step)], preferred_element_type=F32)
        for k in range(tp_count):
            own = slice(k * count, (k + 1) * count)
            outs[k][:, pl.ds(at, step)] = mixed[own].astype(BF16)
            outs[k][:, pl.ds(width + at, step)] = shared[own].astype(BF16)
        return unused

    lax.fori_loop(0, width // step, columns_of, 0)


def combine_kernel(top, cap, tp_count, group, blocks, *refs):
    plane = CORES * tp_count
    back, facts = refs[:plane], refs[plane]
    outs = refs[plane + 1 : plane + 1 + 2 * blocks]
    held, high, low = refs[plane + 1 + 2 * blocks :]
    per_place = blocks * cap
    for j in range(plane):
        held[j * per_place : (j + 1) * per_place, :] = back[j][
            group * per_place : (group + 1) * per_place, :
        ]
    count, half = outs[0].shape
    lane = lax.broadcasted_iota(I32, (count, plane * per_place), 1)
    for b in range(blocks):
        known = facts[pl.ds((group * blocks + b) * count, count), :].astype(F32)
        row = slot_rows(known, b, top, cap, per_place, tp_count)
        most = jnp.zeros(lane.shape, F32)
        rest = jnp.zeros(lane.shape, F32)
        for k in range(top):
            hit = lane == row[:, k : k + 1]
            most = jnp.where(hit, known[:, 2 * top + k : 2 * top + k + 1], most)
            rest = jnp.where(hit, known[:, 3 * top + k : 3 * top + k + 1], rest)
        high[pl.ds(b * count, count), :] = most.astype(BF16)
        low[pl.ds(b * count, count), :] = rest.astype(BF16)
    step = 512
    for h in range(2):

        def columns(n, unused):
            at = pl.multiple_of(n * step, step)
            rows = held[:, pl.ds(h * half + at, step)]
            part = jnp.dot(high[...], rows, preferred_element_type=F32)
            part = part + jnp.dot(low[...], rows, preferred_element_type=F32)
            part = part.astype(BF16)
            for b in range(blocks):
                outs[2 * b + h][:, pl.ds(at, step)] = part[b * count : (b + 1) * count]
            return unused

        lax.fori_loop(0, half // step, columns, 0)


def plane_exchange(pieces, chips, tp_count):
    whole = [(z, core, i) for z in range(chips) for core in range(CORES) for i in range(tp_count)]

    def moved(piece, across, along):
        pairs = [
            (
                (z * CORES + core) * tp_count + i,
                (z * CORES + (core ^ across)) * tp_count + (i + along) % tp_count,
            )
            for z, core, i in whole
        ]
        return lax.ppermute(piece, ("z", "core", "tp"), pairs)

    middle = tp_count // 2
    halfway = [moved(pieces[middle], 0, 1), moved(pieces[tp_count + middle], 0, -1)]
    got = {0: pieces[0]}
    for along in (1, tp_count - 1):
        for across in range(CORES):
            got[across * tp_count + along] = moved(pieces[across * tp_count + along], across, along)
    got[tp_count] = moved(pieces[tp_count], 1, 0)
    got[middle] = moved(halfway[0], 0, middle - 1)
    got[tp_count + middle] = moved(halfway[1], 1, 1 - middle)
    return [got[j] for j in range(CORES * tp_count)]


def rms_scale(values, gains):
    return values * lax.rsqrt(jnp.mean(values * values, axis=-1, keepdims=True) + EPSILON) * gains


def on_device(
    outer_gate,
    inner_gate,
    inner_value,
    conv_taps,
    mixer_out,
    mixer_gain,
    moe_tokens,
    expert_gain,
    route_ids,
    route_weights,
    expert_gate,
    expert_up,
    expert_down,
    shared_gate,
    shared_up,
    shared_down,
):
    chips, tp_count = lax.axis_size("z"), lax.axis_size("tp")
    plane = CORES * tp_count
    tp = lax.axis_index("tp")
    row_count, width = moe_tokens.shape
    top = route_ids.shape[1]
    half = width // 2
    expert_count = chips * plane
    cap = (3 * row_count * top + 2 * expert_count - 1) // (2 * expert_count)
    reach = chips // 2
    far = chips - reach - 1

    left, right, normed, last = on_core(
        prepare_kernel,
        [AUTO] * 4 + [HBM] * 2,
        [
            ((row_count, half + LANES), BF16, VMEM),
            ((row_count, half), BF16, VMEM),
            ((row_count, width), BF16, VMEM),
            ((16, inner_gate.shape[1]), BF16, VMEM),
        ],
        moe_tokens,
        expert_gain.reshape(1, width),
        route_ids.T,
        route_weights.T,
        inner_gate,
        inner_value,
        scratch=[pltpu.SemaphoreType.DMA((2,))],
        limit=56,
    )

    near = [normed] + [lax.ppermute(normed, "tp", ring(tp_count, k)) for k in range(1, tp_count)]
    pairs = [(i, i + 1) for i in range(chips * CORES - 1)]
    before = lax.ppermute(last, ("z", "core"), pairs)

    rise, fall = ring(chips, 1), ring(chips, -1)
    got = {("u", 0): (left, right), ("d", 0): (left, right)}
    order = [("u", 0)]
    for s in range(1, far + 1):
        if s == SIDE_STEP:
            near, before, got["u", s - 1] = lax.optimization_barrier(
                (near, before, got["u", s - 1])
            )
        pairs = [
            lax.optimization_barrier((lax.ppermute(up, "z", rise), lax.ppermute(down, "z", fall)))
            for up, down in zip(got["u", s - 1], got["d", s - 1])
        ]
        got["u", s], got["d", s] = zip(*pairs)
        order += [("u", s), ("d", s)]
    got["u", reach] = (
        lax.ppermute(got["u", far][0], "z", rise),
        lax.ppermute(got["d", far][1], "z", fall),
    )
    order.append(("u", reach))

    groups = 2
    blocks = chips // groups
    rows = chips * cap
    lefts = [got[n][0] for n in order]
    rights = [got[n][1] for n in order]
    *slots, facts = on_core(
        functools.partial(pick_kernel, top, cap, tp_count, groups, blocks),
        [VMEM] * (2 * chips),
        [((rows, width), BF16, VMEM)] * plane + [((chips * row_count, LANES), BF16, VMEM)],
        *lefts,
        *rights,
        scratch=[
            pltpu.VMEM((chips * row_count, width), BF16),
            pltpu.VMEM((groups, plane * blocks * cap, blocks * row_count), BF16),
        ],
        limit=12,
    )
    here = plane_exchange(slots, chips, tp_count)
    hidden = expert_gate.shape[2]
    result = on_core(
        functools.partial(expert_kernel, plane, rows),
        [VMEM] * plane + [HBM] * 3,
        [((rows, width), BF16, VMEM)] * plane,
        *here,
        expert_gate,
        expert_up,
        expert_down,
        scratch=[
            pltpu.VMEM((plane * rows, width), BF16),
            pltpu.VMEM((plane * rows, hidden), BF16),
            pltpu.VMEM((width, hidden), BF16),
            pltpu.VMEM((width, hidden), BF16),
            pltpu.VMEM((hidden, width), BF16),
            pltpu.SemaphoreType.DMA((3,)),
        ],
        limit=EXPERT_LIMIT,
    )
    turned = [result[a * tp_count + -k % tp_count] for a in range(CORES) for k in range(tp_count)]
    turned = plane_exchange(turned, chips, tp_count)
    back = [turned[a * tp_count + -k % tp_count] for a in range(CORES) for k in range(tp_count)]

    columns = inner_gate.shape[1]
    both = on_core(
        functools.partial(sides_kernel, tp_count),
        [VMEM] * (9 + tp_count),
        [((row_count, 2 * width), BF16, VMEM)] * tp_count,
        outer_gate,
        inner_gate,
        inner_value,
        before,
        conv_taps,
        mixer_out,
        *near,
        shared_gate,
        shared_up,
        shared_down,
        scratch=[
            pltpu.VMEM((inner_gate.shape[0] + 8, columns), F32),
            pltpu.VMEM((inner_gate.shape[0], columns), BF16),
            pltpu.VMEM((tp_count * row_count, width), BF16),
        ],
        limit=10,
    )

    both, back = lax.optimization_barrier((list(both), back))
    parts = {}
    for g in reversed(range(groups)):
        done = on_core(
            functools.partial(combine_kernel, top, cap, tp_count, g, blocks),
            [VMEM] * (plane + 1),
            [((row_count, half), BF16, VMEM)] * (2 * blocks),
            *back,
            facts,
            scratch=[
                pltpu.VMEM((plane * blocks * cap, width), BF16),
                pltpu.VMEM((blocks * row_count, plane * blocks * cap), BF16),
                pltpu.VMEM((blocks * row_count, plane * blocks * cap), BF16),
            ],
            limit=10,
        )
        for b, n in enumerate(order[g * blocks : (g + 1) * blocks]):
            parts[n] = (done[2 * b], done[2 * b + 1])

    total = both[0].astype(F32)
    rising = [parts["u", reach][0], parts["d", far][1]]
    falling = [parts["u", far][0], parts["u", reach][1]]
    for s in range(reach, 0, -1):
        for h in range(2):
            first_up, first_down = (reach, far) if h == 0 else (far, reach)
            if s <= first_up:
                rising[h] = lax.ppermute(rising[h], "z", rise)
                if s > 1:
                    rising[h] = rising[h] + parts["d", s - 1][h]
            if s <= first_down:
                falling[h] = lax.ppermute(falling[h], "z", fall)
                if s > 1:
                    falling[h] = falling[h] + parts["u", s - 1][h]
            if 1 < s < reach:
                rising[h], falling[h] = lax.optimization_barrier((rising[h], falling[h]))
        if s == reach:
            rising[0], falling[1] = lax.optimization_barrier((rising[0], falling[1]))
        k = reach - EXCHANGE_STEP - s
        if 1 <= k < tp_count:
            both[k], rising[0] = lax.optimization_barrier((both[k], rising[0]))
            total = total + lax.ppermute(both[k], "tp", ring(tp_count, k)).astype(F32)
    sums = [
        rising[h].astype(F32) + falling[h].astype(F32) + parts["u", 0][h].astype(F32)
        for h in range(2)
    ]
    mixed_rows = rms_scale(total[:, :width], mixer_gain).astype(BF16)
    shared = total[:, width:]
    expert_rows = (shared + jnp.concatenate(sums, axis=1)).astype(BF16)
    return (mixed_rows, expert_rows)


def solution(mesh):
    sizes = dict(mesh.shape)
    sizes = (sizes["grp"], sizes["ep"] // CORES, CORES, sizes["tp"])
    fine = jax.sharding.Mesh(mesh.devices.reshape(sizes), ("grp", "z", "core", "tp"))
    sequence = P(("grp", "z", "core"), "tp")
    tokens = P(("grp", "z", "core", "tp"), None)
    experts = P(("z", "core", "tp"), None, None)
    return jax.shard_map(
        on_device,
        mesh=fine,
        in_specs=(
            sequence,
            sequence,
            sequence,
            P(),
            P("tp", None),
            P(),
            tokens,
            P(),
            tokens,
            tokens,
            experts,
            experts,
            experts,
            P(None, "tp"),
            P(None, "tp"),
            P("tp", None),
        ),
        out_specs=(tokens, tokens),
        check_vma=False,
    )
```
